256 devices in a mesh: sp: 16 (over y, x), tp: 16 (over z, core).
Axes of the slice: x: 4, y: 4, z: 8, core: 2. Of those that a mesh axis runs over, the one named last changes fastest.
Arguments:
- conv_outer: bfloat16 [2048, 4096], P('tp', 'sp'), may hold values from -6 to 6
- conv_inner: bfloat16 [2048, 4096], P('tp', 'sp'), may hold values from -6 to 6
- conv_input: bfloat16 [2048, 4096], P('tp', 'sp'), may hold values from -6 to 6
- conv_taps: float32 [3, 2048], P(None, 'tp'), may hold values from -3 to 3
- out_proj: bfloat16 [2048, 4096], P('tp'), may hold values from -0.125 to 0.125
- mixed_state: bfloat16 [4096, 4096], P('sp', 'tp'), may hold values from -6 to 6
- route_ids: int32 [4096, 2], P('sp'), may hold values from 0 to 15, all different within a row; in each aligned block of 256 rows (0 to 255, 256 to 511, ...) at most 64 rows name the same one
- route_weights: float32 [4096, 2], P('sp'), may hold values from 0.1 to 1
- w_gate: bfloat16 [16, 2048, 4096], P('sp', 'tp'), may hold values from -0.09375 to 0.09375
- w_up: bfloat16 [16, 2048, 4096], P('sp', 'tp'), may hold values from -0.09375 to 0.09375
- w_down: bfloat16 [16, 2048, 4096], P('sp', 'tp'), may hold values from -0.125 to 0.125
- cotangent: bfloat16 [4096, 4096], P('sp', 'tp'), may hold values from -8 to 8
Outputs:
- grad_gate: float32 [16, 2048, 4096], P('sp', 'tp')
- grad_up: float32 [16, 2048, 4096], P('sp', 'tp')
- grad_down: float32 [16, 2048, 4096], P('sp', 'tp')
- grad_mixed: bfloat16 [4096, 4096], P('sp', 'tp')
- grad_proj: float32 [2048, 4096], P('tp', 'sp')
- grad_outer: bfloat16 [2048, 4096], P('tp', 'sp')
- grad_inner: bfloat16 [2048, 4096], P('tp', 'sp')
- grad_input: bfloat16 [2048, 4096], P('tp', 'sp')
The draws below stay inside these ranges and needn't reach their ends.
Inputs may be any that keep to these rules, and one draw needn't show every extreme that they name: `route_ids`: each row names 2 different experts; among the tokens of one index of sp no expert is named more than 64 times, a bound that some block reaches.
All inputs are finite; a program needn't handle non-finite values.
Results may differ from the reference program's by a relative error of at most 0.022.
Values may be sent and summed in bfloat16 or wider, within the bound.
No kernel may reach another device: no remote copies, remote signals or barrier semaphores. Data moves between devices by JAX's collectives and lax.ppermute only.
A program may use at most 128 MiB of HBM per device.

```python
import math
import jax
import jax.numpy as jnp
import numpy as np
from jax import lax

D = 4096
FF = 2048
CH = 2048
TAPS = 3
TOP = 2
TOK_DEV = 256
EXPERTS = 16
CAP = 64
TOKENS = 4096
N_SP = 16
N_TP = 16


def with_spikes(result, rng, source, target, blocks, factor):
    def block_of(dim):
        return (jnp.arange(result.shape[dim]) // (result.shape[dim] // blocks)).reshape((-1,) + (1,) * (result.ndim - 1 - dim))

    near = jax.random.permutation(rng, blocks)[block_of(target)]
    other_side = (block_of(target) + blocks // 2) % blocks
    return jnp.where((block_of(source) == near) | (block_of(source) == other_side), factor * result, result)


def level_of(stream_key, dims, cuts, least, top_value):
    def one(axis_at, shards_of):
        heights = jax.random.uniform(jax.random.fold_in(jax.random.fold_in(stream_key, 6), axis_at), (shards_of,), jnp.float32, least / len(cuts), top_value / len(cuts))
        return jnp.repeat(jnp.exp(heights), dims[axis_at] // shards_of).reshape((-1,) + (1,) * (len(dims) - axis_at - 1))

    factor_of = one(*cuts[0])
    for cut in cuts[1:]:
        factor_of = factor_of * one(*cut)
    return factor_of


def shared_out(stream_key, own, number, rows, amount, top, most, lean):
    ranking = jax.random.permutation(stream_key, amount)
    packed, ordinary = load_shares(amount, rows * top, most, lean, True), load_shares(amount, rows * top, most, lean, False)
    places = jnp.arange(amount)

    def named(lengths, rotation):
        used = int((lengths > 0).sum())
        fixed = max(1, used // 4)
        shifted = fixed + (places - fixed + rotation * (used - fixed)) % max(1, amount - fixed)
        return jnp.zeros((amount,), jnp.int32).at[ranking[jnp.where(places < fixed, places, shifted)]].set(jnp.asarray(lengths, jnp.int32))

    lengths = jnp.where(number % 4 == 0, named(packed, number // 4), named(ordinary, number - number // 4 - 1))
    mixed = jax.random.permutation(jax.random.fold_in(own, 3), amount)
    giver, taker = mixed[0:amount // 2 * 2:2], mixed[1:amount // 2 * 2:2]
    margin = jnp.minimum(lengths[giver] - 1, most - lengths[taker]) // 2
    margin = jnp.where((giver == ranking[0]) | (taker == ranking[0]) | (lengths[taker] == 0), 0, jnp.maximum(margin, 0))
    shifted = jax.random.randint(jax.random.fold_in(own, 4), (amount // 2,), 0, 1 << 20) % (margin + 1)
    lengths = lengths.at[giver].add(-shifted).at[taker].add(shifted)
    items = jnp.searchsorted(jnp.cumsum(lengths), jnp.arange(rows * top), side="right").astype(jnp.int32)
    grid = items.reshape(top, rows).T
    grid = grid[jax.random.permutation(jax.random.fold_in(own, 1), rows)]
    rotation = jax.random.randint(jax.random.fold_in(own, 2), (rows, 1), 0, top)
    return jnp.take_along_axis(grid, (jnp.arange(top)[None, :] + rotation) % top, axis=1)


def load_shares(number_of, total, most, slope, full):
    loads = [(1 << 20) // math.isqrt(standing ** slope) + 1 for standing in range(1, number_of + 1)]
    largest = most if full else min(most, max(-(-total // number_of), total * loads[0] // sum(loads)))
    least = 1 if total - largest >= number_of - 1 else 0
    holding, surplus = [largest] + [least] * (number_of - 1), total - largest - least * (number_of - 1)
    while surplus > 0:
        free = [i for i in range(1, number_of) if holding[i] < largest] or [i for i in range(1, number_of) if holding[i] < most]
        pool, left = sum([loads[i] for i in free]), surplus
        for i in free:
            extra = min(most - holding[i], max(1, left * loads[i] // pool), surplus)
            holding[i] = holding[i] + extra
            surplus = surplus - extra
    return np.array(holding)


def centred(key, extent, scale, limit, split=(), kind=jnp.bfloat16):
    values = jax.random.normal(key, extent, jnp.float32) * scale
    if len(split) > 0:
        values = level_of(key, extent, split, -0.22, 0.18) * values
    return jnp.clip(values, min=-limit, max=limit).astype(kind)


def noise_with(key, shape, spread, most, split, heavy, held_as=jnp.bfloat16):
    drawn = spread * jax.random.normal(key, shape, jnp.float32)
    if split:
        drawn = drawn * level_of(key, shape, split, -0.22, 0.18)
    return jnp.clip(with_spikes(drawn, jax.random.fold_in(key, 3), *heavy), -most, most).astype(held_as)


def setup_inputs(seed: int = 0) -> dict:
    arg_keys = jax.random.split(jax.random.key(seed), 13)
    conv_outer = centred(arg_keys[0], (CH, TOKENS), 1.0, 6.0, ((0, 16), (1, 16)))
    conv_inner = centred(arg_keys[1], (CH, TOKENS), 1.0, 6.0, ((0, 16), (1, 16)))
    conv_input = centred(arg_keys[2], (CH, TOKENS), 1.0, 6.0, ((0, 16), (1, 16)))
    conv_taps = centred(arg_keys[3], (TAPS, CH), 0.6, 3.0, ((1, 16),), jnp.float32)
    out_proj = centred(arg_keys[4], (CH, D), CH ** -0.5, 0.125, ((0, 16),))
    mixed_state = centred(arg_keys[5], (TOKENS, D), 1.0, 6.0, ((0, 16), (1, 16)))
    route_ids_keys = jax.random.split(jax.random.fold_in(arg_keys[6], 1), TOKENS // TOK_DEV)
    route_ids_turns = jax.random.permutation(jax.random.fold_in(arg_keys[6], 3), TOKENS // TOK_DEV)
    route_ids = jax.vmap(lambda own, number: shared_out(jax.random.fold_in(arg_keys[6], 2), own, number, TOK_DEV, EXPERTS, TOP, CAP, 2))(route_ids_keys, route_ids_turns).reshape((TOKENS, TOP))
    route_weights = jnp.clip(0.1 + 0.9 * jax.random.uniform(arg_keys[7], (TOKENS, TOP), jnp.float32) ** level_of(arg_keys[7], (TOKENS, TOP), ((0, 16),), -0.2, 0.2), 0.1, 1.0)
    w_gate = centred(arg_keys[8], (EXPERTS, FF, D), D ** -0.5, 0.09375, ((0, 16), (1, 16)))
    w_up = centred(arg_keys[9], (EXPERTS, FF, D), D ** -0.5, 0.09375, ((0, 16), (1, 16)))
    w_down = centred(arg_keys[10], (EXPERTS, FF, D), FF ** -0.5, 0.125, ((0, 16), (1, 16)))
    cotangent = noise_with(arg_keys[11], (TOKENS, D), 1.0, 8.0, ((0, 16), (1, 16)), (0, 1, 16, 2.0))
    return {"conv_outer": conv_outer, "conv_inner": conv_inner, "conv_input": conv_input, "conv_taps": conv_taps, "out_proj": out_proj, "mixed_state": mixed_state, "route_ids": route_ids, "route_weights": route_weights, "w_gate": w_gate, "w_up": w_up, "w_down": w_down, "cotangent": cotangent}


def expert_core(rows_in, rows_grad, gate_w, up_w, down_w):
    gate_pre = jnp.dot(rows_in, gate_w.T, preferred_element_type=jnp.float32)
    up_pre = jnp.dot(rows_in, up_w.T, preferred_element_type=jnp.float32)
    sig_gate = jax.nn.sigmoid(gate_pre)
    silu_gate = gate_pre * sig_gate
    hidden = (silu_gate * up_pre).astype(jnp.bfloat16)
    back_hidden = jnp.dot(rows_grad, down_w.T, preferred_element_type=jnp.float32)
    back_gate = (back_hidden * up_pre * sig_gate * (1.0 + gate_pre * (1.0 - sig_gate))).astype(jnp.bfloat16)
    back_up = (back_hidden * silu_gate).astype(jnp.bfloat16)
    grad_down_e = jnp.dot(hidden.T, rows_grad, preferred_element_type=jnp.float32)
    grad_gate_e = jnp.dot(back_gate.T, rows_in, preferred_element_type=jnp.float32)
    grad_up_e = jnp.dot(back_up.T, rows_in, preferred_element_type=jnp.float32)
    return back_gate, back_up, grad_gate_e, grad_up_e, grad_down_e


def reference(conv_outer, conv_inner, conv_input, conv_taps, out_proj, mixed_state, route_ids, route_weights, w_gate, w_up, w_down, cotangent):
    block_ids = route_ids.reshape(N_SP, TOP * TOK_DEV)
    onehot = (block_ids[:, :, None] == jnp.arange(EXPERTS, dtype=jnp.int32)[None, None, :]).astype(jnp.int32)
    position = jnp.sum(jnp.cumsum(onehot, axis=1) * onehot, axis=2) - 1
    device_ids = jnp.broadcast_to(jnp.arange(N_SP, dtype=jnp.int32)[:, None], block_ids.shape)
    assign = jnp.arange(N_SP * TOP * TOK_DEV, dtype=jnp.int32).reshape(N_SP, TOP * TOK_DEV)
    table = jnp.full((EXPERTS, N_SP, CAP), -1, jnp.int32).at[block_ids, device_ids, position].set(assign)
    table = table.reshape(EXPERTS, N_SP * CAP)
    weight_flat = route_weights.reshape(-1)

    def expert_pass(operands):
        table_row, gate_w, up_w, down_w = operands
        valid = table_row >= 0
        safe_idx = jnp.where(valid, table_row, 0)
        token_idx = safe_idx // TOP
        rows_in = jnp.where(valid[:, None], mixed_state[token_idx], jnp.zeros((), jnp.bfloat16))
        scale = jnp.where(valid, weight_flat[safe_idx], jnp.zeros((), jnp.float32))
        rows_grad = (cotangent[token_idx].astype(jnp.float32) * scale[:, None]).astype(jnp.bfloat16)
        back_gate, back_up, grad_gate_e, grad_up_e, grad_down_e = expert_core(rows_in, rows_grad, gate_w, up_w, down_w)
        row_count = rows_in.shape[0]
        gate_blocks = back_gate.astype(jnp.float32).reshape(row_count, N_TP, FF // N_TP)
        up_blocks = back_up.astype(jnp.float32).reshape(row_count, N_TP, FF // N_TP)
        gate_wblk = gate_w.astype(jnp.float32).reshape(N_TP, FF // N_TP, D)
        up_wblk = up_w.astype(jnp.float32).reshape(N_TP, FF // N_TP, D)
        partial_value = jnp.einsum("rbf,bfd->brd", gate_blocks, gate_wblk) + jnp.einsum("rbf,bfd->brd", up_blocks, up_wblk)
        rounded = lax.optimization_barrier(partial_value.astype(jnp.bfloat16))
        row_back = jnp.sum(rounded.astype(jnp.float32), axis=0).astype(jnp.bfloat16)
        return row_back, grad_gate_e, grad_up_e, grad_down_e

    row_back, grad_gate, grad_up, grad_down = lax.map(expert_pass, (table, w_gate, w_up, w_down))
    flat_table = table.reshape(-1)
    valid_all = flat_table >= 0
    token_all = jnp.where(valid_all, flat_table, 0) // TOP
    back_vals = jnp.where(valid_all[:, None], row_back.reshape(-1, D).astype(jnp.float32), jnp.zeros((), jnp.float32))
    moe_grad = jnp.zeros((TOKENS, D), jnp.float32).at[token_all].add(back_vals)
    grad_mixed = (cotangent.astype(jnp.float32) + moe_grad).astype(jnp.bfloat16)

    inner_prod = conv_inner.astype(jnp.float32) * conv_input.astype(jnp.float32)
    padded = jnp.pad(inner_prod, ((0, 0), (TAPS - 1, 0)))
    conv_out = jnp.zeros_like(inner_prod)
    for offset in range(TAPS):
        conv_out = conv_out + conv_taps[offset][:, None] * padded[:, offset:offset + TOKENS]
    mixer_act = (conv_outer.astype(jnp.float32) * conv_out).astype(jnp.bfloat16)
    back_mixer = jnp.dot(out_proj, grad_mixed.T, preferred_element_type=jnp.float32)
    grad_proj = jnp.dot(mixer_act, grad_mixed, preferred_element_type=jnp.float32)
    grad_outer = (back_mixer * conv_out).astype(jnp.bfloat16)
    back_conv = back_mixer * conv_outer.astype(jnp.float32)
    padded_back = jnp.pad(back_conv, ((0, 0), (0, TAPS - 1)))
    back_prod = jnp.zeros_like(back_conv)
    for offset in range(TAPS):
        shift_by = TAPS - 1 - offset
        back_prod = back_prod + conv_taps[offset][:, None] * padded_back[:, shift_by:shift_by + TOKENS]
    grad_inner = (back_prod * conv_input.astype(jnp.float32)).astype(jnp.bfloat16)
    grad_input = (back_prod * conv_inner.astype(jnp.float32)).astype(jnp.bfloat16)
    return grad_gate, grad_up, grad_down, grad_mixed, grad_proj, grad_outer, grad_inner, grad_input
```

```python
import functools

import jax
import jax.numpy as jnp
from jax import lax
from jax.experimental import pallas as pl
from jax.experimental.pallas import tpu as pltpu
from jax.sharding import Mesh
from jax.sharding import PartitionSpec as P


TP = ("z", "c")
BF16 = jnp.bfloat16
F32 = jnp.float32


def dot_nn(a, b):
    return lax.dot_general(a, b, (((1,), (0,)), ((), ())), preferred_element_type=F32)


def dot_nt(a, b):
    return lax.dot_general(a, b, (((1,), (1,)), ((), ())), preferred_element_type=F32)


def dot_tn(a, b):
    return lax.dot_general(a, b, (((0,), (0,)), ((), ())), preferred_element_type=F32)


def cost(flops, nbytes):
    return pl.CostEstimate(flops=int(flops), bytes_accessed=int(nbytes), transcendentals=0)


def route_kernel(experts, cap, ids_ref, wts_ref, state_ref, sent_ref, pick_ref, scale_ref):
    tokens = ids_ref.shape[1]
    first, second = ids_ref[0:1, :], ids_ref[1:2, :]
    expert = lax.broadcasted_iota(jnp.int32, (experts, tokens), 0)
    is_first, is_second = first == expert, second == expert
    named = jnp.logical_or(is_first, is_second)
    before = lax.broadcasted_iota(jnp.int32, (tokens, tokens), 0) < lax.broadcasted_iota(
        jnp.int32, (tokens, tokens), 1
    )
    earlier = dot_nn(named.astype(F32).astype(BF16), before.astype(F32).astype(BF16))
    slot = jnp.where(named, earlier.astype(jnp.int32), -1)
    weight = jnp.where(is_first, wts_ref[0:1, :], jnp.where(is_second, wts_ref[1:2, :], 0.0))
    place = lax.broadcasted_iota(jnp.int32, (cap, tokens), 0)
    for e in range(experts):
        hit = slot[e : e + 1, :] == place
        pick_ref[e * cap : (e + 1) * cap, :] = hit.astype(F32).astype(BF16)
        taken = jnp.sum(jnp.where(hit, weight[e : e + 1, :], 0.0), axis=1, keepdims=True)
        scale_ref[e * cap : (e + 1) * cap, :] = jnp.broadcast_to(taken, (cap, 128))
    sent_ref[...] = dot_nn(pick_ref[...], state_ref[...]).astype(BF16)


def spread_kernel(pick_ref, scale_ref, *refs):
    pieces, (low_ref, high_ref) = refs[:-2], refs[-2:]
    width = pieces[0].shape[1]
    half = len(pieces) // 2
    scale = scale_ref[:, 0:1]
    for j, piece in enumerate(pieces):
        rows = (dot_nn(pick_ref[...], piece[...]) * scale).astype(BF16)
        out = low_ref if j < half else high_ref
        out[:, (j % half) * width : (j % half + 1) * width] = rows


def expert_kernel(
    slab_ref, state_ref, ml_ref, mh_ref, tl_ref, th_ref, wg_ref, wu_ref, wd_ref, part_ref, act_ref, wgu_ref
):
    slabs, width = state_ref.shape[0], state_ref.shape[2]
    hidden_n = wd_ref.shape[0]

    @pl.when(pl.program_id(0) == 0)
    def _():
        wgu_ref[:hidden_n] = wg_ref[...]
        wgu_ref[hidden_n:] = wu_ref[...]

    rows = jnp.concatenate([state_ref[s] for s in range(slabs)], axis=1)
    pre = dot_nt(rows, wgu_ref[...])
    gate_pre, up_pre = pre[:, :hidden_n], pre[:, hidden_n:]
    back_hidden = jnp.zeros(gate_pre.shape, F32)
    per = ml_ref.shape[1] // width
    for q, ref in enumerate((ml_ref, mh_ref, tl_ref, th_ref)):
        pieces = [
            wd_ref[:, pl.ds(pl.multiple_of(slab_ref[q * per + j] * width, width), width)]
            for j in range(per)
        ]
        back_hidden = back_hidden + dot_nt(ref[...], jnp.concatenate(pieces, axis=1))
    sig_gate = jax.nn.sigmoid(gate_pre)
    silu_gate = gate_pre * sig_gate
    hidden = (silu_gate * up_pre).astype(BF16)
    back_gate = (back_hidden * up_pre * sig_gate * (1.0 + gate_pre * (1.0 - sig_gate))).astype(BF16)
    back_up = (back_hidden * silu_gate).astype(BF16)
    back = jnp.concatenate([back_gate, back_up], axis=1)
    act_ref[:, : 2 * hidden_n] = back
    act_ref[:, 2 * hidden_n :] = hidden
    for s in range(slabs):
        part_ref[s] = dot_nn(back, wgu_ref[:, s * width : (s + 1) * width]).astype(BF16)


def weight_grad_kernel(slab_ref, act_ref, state_ref, ml_ref, mh_ref, tl_ref, th_ref, gg_ref, gu_ref, gd_ref):
    hidden_n = gg_ref.shape[0]
    step, per = pl.program_id(0), pl.num_programs(0) // 4
    both = dot_tn(act_ref[:, : 2 * hidden_n], state_ref[0])
    gg_ref[...] = both[:hidden_n]
    gu_ref[...] = both[hidden_n:]
    for q, ref in enumerate((ml_ref, mh_ref, tl_ref, th_ref)):

        @pl.when(step // per == q)
        def _(ref=ref):
            gd_ref[...] = dot_tn(act_ref[:, 2 * hidden_n :], ref[...])


def combine_kernel(pick_ref, rows_ref, cot_ref, out_ref):
    total = dot_tn(pick_ref[...], rows_ref[...])
    out_ref[...] = (cot_ref[...].astype(F32) + total).astype(BF16)


def proj_kernel(slab_ref, act_ref, *refs):
    pieces, out_ref = refs[:-1], refs[-1]
    for j, piece in enumerate(pieces):
        out_ref[slab_ref[j]] = dot_nn(act_ref[...], piece[...]).astype(BF16)


def mixer_kernel(slab_ref, proj_ref, conv_ref, outer_ref, *refs):
    pieces, (grad_ref, back_ref) = refs[:-2], refs[-2:]
    width = pieces[0].shape[1]
    back = jnp.zeros(back_ref.shape, F32)
    for j, piece in enumerate(pieces):
        start = pl.multiple_of(slab_ref[j] * width, width)
        back = back + dot_nt(proj_ref[:, pl.ds(start, width)], piece[...])
    grad_ref[...] = (back * conv_ref[...]).astype(BF16)
    back_ref[...] = back * outer_ref[...].astype(F32)


def ring_steps(size):
    steps = [0]
    for k in range(1, size // 2):
        steps += [k, -k]
    return steps + [size // 2]


def gathered(value, axis):
    size = lax.axis_size(axis)
    pieces = [value]
    for k in ring_steps(size)[1:]:
        pieces.append(lax.ppermute(value, axis, [(i, (i + k) % size) for i in range(size)]))
    return pieces


def from_behind(value, axis, steps):
    count = lax.axis_size(axis)
    first, last = (max(0, -steps), min(count, count - steps))
    return lax.ppermute(value, axis, [(source, source + steps) for source in range(first, last)])


def shards(
    conv_outer,
    conv_inner,
    conv_input,
    conv_taps,
    out_proj,
    mixed_state,
    route_ids,
    route_weights,
    w_gate,
    w_up,
    w_down,
    cotangent,
):
    tok_count, width = mixed_state.shape
    sp_size = lax.axis_size("sp")
    z_size = lax.axis_size("z")
    slabs = 2 * z_size
    local_experts, hidden_n, features = w_gate.shape
    experts = local_experts * sp_size
    cap = 4 * tok_count // experts
    slots = experts * cap
    core, place = lax.axis_index("c"), lax.axis_index("z")
    origin = (place - jnp.array(ring_steps(z_size), jnp.int32)) % z_size
    slab_of = jnp.concatenate([2 * origin + core, 2 * origin + 1 - core]).astype(jnp.int32)
    shape = jax.ShapeDtypeStruct

    cot_pieces = gathered(cotangent, "z")

    sent_state, pick, scale = pl.pallas_call(
        functools.partial(route_kernel, experts, cap),
        out_shape=(
            shape((slots, width), BF16),
            shape((slots, tok_count), BF16),
            shape((slots, 128), F32),
        ),
        cost_estimate=cost(2 * slots * tok_count * width, 4 * slots * width),
        name="route",
    )(route_ids.T, route_weights.T, mixed_state)
    recv_state = lax.all_to_all(
        sent_state.reshape(experts, cap, width), "sp", split_axis=0, concat_axis=0, tiled=True
    )
    state_all = lax.all_gather(recv_state.reshape(slots, width), TP, axis=0, tiled=False)

    half = z_size // 2 * width
    cot_low, cot_high = pl.pallas_call(
        spread_kernel,
        out_shape=(shape((slots, half), BF16),) * 2,
        cost_estimate=cost(4 * slots * tok_count * half, 8 * slots * half),
        name="spread",
    )(pick, scale, *cot_pieces)
    swap = [(0, 1), (1, 0)]

    def exchanged(part):
        got = lax.all_to_all(
            part.reshape(experts, cap, half), "sp", split_axis=0, concat_axis=0, tiled=True
        ).reshape(slots, half)
        return got, lax.ppermute(got, "c", swap)

    my_low, their_low = exchanged(cot_low)
    my_high, their_high = exchanged(cot_high)
    cots = (my_low, my_high, their_low, their_high)

    block = 256
    whole = lambda *dims: pl.BlockSpec(dims, lambda *_: (0,) * len(dims))
    cot_rows = pl.BlockSpec((block, half), lambda r, core: (r, 0))
    partial_value, acts = pl.pallas_call(
        expert_kernel,
        grid_spec=pltpu.PrefetchScalarGridSpec(
            num_scalar_prefetch=1,
            grid=(slots // block,),
            in_specs=[
                pl.BlockSpec((slabs, block, width), lambda r, core: (0, r, 0)),
                *[cot_rows] * 4,
                *[whole(hidden_n, features)] * 3,
            ],
            out_specs=[
                pl.BlockSpec((slabs, block, width), lambda r, core: (0, r, 0)),
                pl.BlockSpec((block, 3 * hidden_n), lambda r, core: (r, 0)),
            ],
            scratch_shapes=[pltpu.VMEM((2 * hidden_n, features), BF16)],
        ),
        out_shape=(shape((slabs, slots, width), BF16), shape((slots, 3 * hidden_n), BF16)),
        cost_estimate=cost(10 * slots * hidden_n * features, 6 * slots * features),
        name="expert",
    )(slab_of, state_all, *cots, w_gate[0], w_up[0], w_down[0])

    row_back = lax.psum_scatter(partial_value, TP, scatter_dimension=0, tiled=False)

    quarter = slabs // 4

    def cot_piece(q):
        return pl.BlockSpec(
            (slots, width), lambda s, core: (0, jnp.clip(s - q * quarter, 0, quarter - 1))
        )

    grad_out = pl.BlockSpec((hidden_n, width), lambda s, slab: (0, slab[s]))
    grad_gate, grad_up, grad_down = pl.pallas_call(
        weight_grad_kernel,
        grid_spec=pltpu.PrefetchScalarGridSpec(
            num_scalar_prefetch=1,
            grid=(slabs,),
            in_specs=[
                whole(slots, 3 * hidden_n),
                pl.BlockSpec((1, slots, width), lambda s, slab: (slab[s], 0, 0)),
                *[cot_piece(q) for q in range(4)],
            ],
            out_specs=[grad_out] * 3,
        ),
        out_shape=(shape((hidden_n, features), F32),) * 3,
        cost_estimate=cost(6 * slots * hidden_n * features, 6 * slots * features),
        name="weight_grads",
    )(slab_of, acts, state_all, *cots)
    row_back, grad_gate, grad_up, grad_down = lax.optimization_barrier(
        (row_back, grad_gate, grad_up, grad_down)
    )

    arrived = lax.all_to_all(
        row_back.reshape(experts, cap, width), "sp", split_axis=0, concat_axis=0, tiled=True
    ).reshape(slots, width)
    grad_mixed = pl.pallas_call(
        combine_kernel,
        out_shape=shape((tok_count, width), BF16),
        cost_estimate=cost(2 * slots * tok_count * width, 4 * slots * width),
        name="combine",
    )(pick, arrived, cotangent)
    near = gathered(grad_mixed, "z")
    full_back = near + [lax.ppermute(piece, "c", swap) for piece in near]

    taps_count = conv_taps.shape[0]
    rim_width = taps_count - 1
    channels = conv_inner.shape[0]
    head_block = from_behind(
        jnp.stack([conv_inner[:, tok_count - rim_width :], conv_input[:, tok_count - rim_width :]]),
        "sp",
        1,
    )
    inner_ext = jnp.concatenate([head_block[0], conv_inner], axis=1).astype(F32)
    input_ext = jnp.concatenate([head_block[1], conv_input], axis=1).astype(F32)
    inner_prod = inner_ext * input_ext
    conv_out = jnp.zeros((channels, tok_count), F32)
    for offset in range(taps_count):
        conv_out = (
            conv_out + conv_taps[offset][:, None] * inner_prod[:, offset : offset + tok_count]
        )
    mixer_act = (conv_outer.astype(F32) * conv_out).astype(BF16)

    vmem, smem = pl.BlockSpec(memory_space=pltpu.VMEM), pl.BlockSpec(memory_space=pltpu.SMEM)
    proj_term = pl.pallas_call(
        proj_kernel,
        in_specs=[smem] + [vmem] * (1 + slabs),
        out_shape=shape((slabs, channels, width), BF16),
        cost_estimate=cost(2 * channels * tok_count * features, 4 * tok_count * features),
        name="proj",
    )(slab_of, mixer_act, *full_back)
    landed = lax.all_to_all(proj_term, "sp", split_axis=0, concat_axis=0, tiled=True)
    grad_proj = jnp.sum(landed.astype(F32), axis=0)
    grad_outer, back_conv = pl.pallas_call(
        mixer_kernel,
        in_specs=[smem] + [vmem] * (3 + slabs),
        out_shape=(shape((channels, tok_count), BF16), shape((channels, tok_count), F32)),
        cost_estimate=cost(2 * channels * tok_count * features, 4 * tok_count * features),
        name="mixer",
    )(slab_of, out_proj, conv_out, conv_outer, *full_back)
    tail_back = from_behind(back_conv[:, :rim_width], "sp", -1)
    back_ext = jnp.concatenate([back_conv, tail_back], axis=1)
    back_prod = jnp.zeros_like(back_conv)
    for offset in range(taps_count):
        shift_by = rim_width - offset
        back_prod = (
            back_prod + conv_taps[offset][:, None] * back_ext[:, shift_by : shift_by + tok_count]
        )
    grad_inner = (back_prod * conv_input.astype(F32)).astype(BF16)
    grad_input = (back_prod * conv_inner.astype(F32)).astype(BF16)
    return (
        grad_gate[None],
        grad_up[None],
        grad_down[None],
        grad_mixed,
        grad_proj,
        grad_outer,
        grad_inner,
        grad_input,
    )


def solution(mesh):
    torus = Mesh(mesh.devices.reshape(mesh.shape["sp"], mesh.shape["tp"] // 2, 2), ("sp", "z", "c"))

    return jax.shard_map(
        shards,
        mesh=torus,
        in_specs=(
            P(TP, "sp"),
            P(TP, "sp"),
            P(TP, "sp"),
            P(None, TP),
            P(TP, None),
            P("sp", TP),
            P("sp", None),
            P("sp", None),
            P("sp", TP, None),
            P("sp", TP, None),
            P("sp", TP, None),
            P("sp", TP),
        ),
        out_specs=(
            P("sp", TP, None),
            P("sp", TP, None),
            P("sp", TP, None),
            P("sp", TP),
            P(TP, "sp"),
            P(TP, "sp"),
            P(TP, "sp"),
            P(TP, "sp"),
        ),
        check_vma=False,
    )
```

```python
import functools

import jax
import jax.numpy as jnp
from jax import lax
from jax.experimental import pallas as pl
from jax.experimental.pallas import tpu as pltpu
from jax.sharding import Mesh
from jax.sharding import PartitionSpec as P


TP = ("z", "c")
BF16 = jnp.bfloat16
F32 = jnp.float32


def dot_nn(a, b):
    return lax.dot_general(a, b, (((1,), (0,)), ((), ())), preferred_element_type=F32)


def dot_nt(a, b):
    return lax.dot_general(a, b, (((1,), (1,)), ((), ())), preferred_element_type=F32)


def dot_tn(a, b):
    return lax.dot_general(a, b, (((0,), (0,)), ((), ())), preferred_element_type=F32)


def grant(mib):
    return pltpu.CompilerParams(vmem_limit_bytes=mib << 20)


def cost(flops, nbytes):
    return pl.CostEstimate(flops=int(flops), bytes_accessed=int(nbytes), transcendentals=0)


def route_kernel(
    experts, cap, early, ids_ref, wts_ref, state_ref, cot_ref, sent_ref, pick_ref, late_ref, scale_ref
):
    tokens = ids_ref.shape[1]
    first, second = ids_ref[0:1, :], ids_ref[1:2, :]
    expert = lax.broadcasted_iota(jnp.int32, (experts, tokens), 0)
    is_first, is_second = first == expert, second == expert
    named = jnp.logical_or(is_first, is_second)
    before = lax.broadcasted_iota(jnp.int32, (tokens, tokens), 0) < lax.broadcasted_iota(
        jnp.int32, (tokens, tokens), 1
    )
    earlier = dot_nn(named.astype(F32).astype(BF16), before.astype(F32).astype(BF16))
    slot = jnp.where(named, earlier.astype(jnp.int32), -1)
    weight = jnp.where(is_first, wts_ref[0:1, :], jnp.where(is_second, wts_ref[1:2, :], 0.0))
    place = lax.broadcasted_iota(jnp.int32, (cap, tokens), 0)
    hits, scales = [], []
    for e in range(experts):
        hit = slot[e : e + 1, :] == place
        hits.append(hit.astype(F32))
        scales.append(jnp.sum(jnp.where(hit, weight[e : e + 1, :], 0.0), axis=1, keepdims=True))
    pick = jnp.concatenate(hits, axis=0).astype(BF16)
    pick_ref[...] = pick
    late_ref[...] = jnp.concatenate([hit[early:] for hit in hits], axis=0).astype(BF16)
    late_scale = jnp.concatenate([taken[early:] for taken in scales], axis=0)
    scale_ref[...] = jnp.broadcast_to(late_scale, scale_ref.shape)
    state_rows = dot_nn(pick, state_ref[...])
    soon = jnp.concatenate([hit[:early] for hit in hits], axis=0).astype(BF16)
    soon_rows = dot_nn(soon, cot_ref[...]) * jnp.concatenate(
        [taken[:early] for taken in scales], axis=0
    )
    both = []
    for e in range(experts):
        both += [state_rows[e * cap : (e + 1) * cap], soon_rows[e * early : (e + 1) * early]]
    sent_ref[...] = jnp.concatenate(both, axis=0).astype(BF16)


def spread_kernel(late_ref, scale_ref, *refs):
    pieces, out_ref = refs[:-1], refs[-1]
    width = pieces[0].shape[1]
    scale = scale_ref[:, 0:1]
    for j, piece in enumerate(pieces):
        rows = (dot_nn(late_ref[...], piece[...]) * scale).astype(BF16)
        out_ref[:, j * width : (j + 1) * width] = rows


def down_columns(slab_ref, base, wd_ref, count, width):
    pieces = [
        wd_ref[:, pl.ds(pl.multiple_of(slab_ref[base + j] * width, width), width)]
        for j in range(count)
    ]
    return jnp.concatenate(pieces, axis=1)


def expert_first_kernel(
    cap,
    early,
    slab_ref,
    state_ref,
    mine_ref,
    their_ref,
    wg_ref,
    wu_ref,
    wdk_ref,
    wd_ref,
    pre_ref,
    acc_ref,
    late_ref,
):
    slabs, width = state_ref.shape[0], state_ref.shape[2]
    hidden_n = wd_ref.shape[0]
    step, steps = pl.program_id(0), pl.num_programs(0)
    rows = jnp.concatenate([state_ref[s] for s in range(slabs)], axis=1)
    weights = jnp.concatenate([wg_ref[...], wu_ref[...], wdk_ref[...]], axis=0)
    acc = dot_nt(rows, weights)

    def down(base):
        at = pl.multiple_of(slab_ref[base + step] * width, width)
        return wd_ref[:, pl.ds(at, width)]

    late = dot_nt(mine_ref[...], down(0)) + dot_nt(their_ref[...], down(2 * steps))

    @pl.when(step == 0)
    def _():
        acc_ref[...] = acc
        late_ref[...] = late

    @pl.when(step > 0)
    def _():
        acc_ref[...] += acc
        late_ref[...] += late

    @pl.when(step == steps - 1)
    def _():
        late_n, own = cap - early, cap + early
        for i in range(acc_ref.shape[0] // own):
            at, to, few = i * own, i * cap, i * late_n
            pre_ref[to : to + cap, : 2 * hidden_n] = acc_ref[at : at + cap, : 2 * hidden_n]
            pre_ref[to : to + early, 2 * hidden_n :] = acc_ref[at + cap : at + own, 2 * hidden_n :]
            pre_ref[to + early : to + cap, 2 * hidden_n :] = late_ref[few : few + late_n]


def expert_second_kernel(
    cap, early, slab_ref, pre_ref, mine_ref, their_ref, wg_ref, wu_ref, wd_ref, part_ref, act_ref, late_ref, w_ref
):
    slabs, width = part_ref.shape[0], part_ref.shape[2]
    hidden_n = wd_ref.shape[0]

    @pl.when(pl.program_id(0) == 0)
    def _():
        w_ref[:hidden_n] = wg_ref[...]
        w_ref[hidden_n:] = wu_ref[...]

    per = mine_ref.shape[1] // width
    late = dot_nt(mine_ref[...], down_columns(slab_ref, per, wd_ref, per, width))
    late = late + dot_nt(their_ref[...], down_columns(slab_ref, 3 * per, wd_ref, per, width))
    late_n = cap - early
    groups = range(pre_ref.shape[0] // cap)
    none = jnp.zeros((early, hidden_n), F32)
    more = jnp.concatenate(
        [x for i in groups for x in (none, late[i * late_n : (i + 1) * late_n])], axis=0
    )
    gate_pre, up_pre = pre_ref[:, :hidden_n], pre_ref[:, hidden_n : 2 * hidden_n]
    back_hidden = pre_ref[:, 2 * hidden_n :] + more
    sig_gate = jax.nn.sigmoid(gate_pre)
    silu_gate = gate_pre * sig_gate
    hidden = silu_gate * up_pre
    back_gate = back_hidden * up_pre * sig_gate * (1.0 + gate_pre * (1.0 - sig_gate))
    back_up = back_hidden * silu_gate
    back = jnp.concatenate([back_gate, back_up], axis=1)
    rounded = back.astype(BF16)
    for s in range(slabs):
        part_ref[s] = dot_nn(rounded, w_ref[:, s * width : (s + 1) * width]).astype(BF16)
    nothing = jnp.zeros((cap, hidden_n), F32)
    wide = jnp.zeros((early, 2 * hidden_n), F32)
    act_ref[:, : 2 * hidden_n] = jnp.concatenate(
        [x for i in groups for x in (back[i * cap : (i + 1) * cap], wide)], axis=0
    ).astype(BF16)
    act_ref[:, 2 * hidden_n :] = jnp.concatenate(
        [x for i in groups for x in (nothing, hidden[i * cap : i * cap + early])], axis=0
    ).astype(BF16)
    late_ref[...] = jnp.concatenate(
        [hidden[i * cap + early : (i + 1) * cap] for i in groups], axis=0
    ).astype(BF16)


def weight_grad_kernel(
    slab_ref, act_ref, late_ref, state_ref, ml_ref, mh_ref, tl_ref, th_ref, gg_ref, gu_ref, gd_ref
):
    hidden_n = gg_ref.shape[0]
    step, per = pl.program_id(0), pl.num_programs(0) // 4
    every = dot_tn(act_ref[...], state_ref[0])
    gg_ref[...] = every[:hidden_n]
    gu_ref[...] = every[hidden_n : 2 * hidden_n]
    for q, ref in enumerate((ml_ref, mh_ref, tl_ref, th_ref)):

        @pl.when(step // per == q)
        def _(ref=ref):
            gd_ref[...] = every[2 * hidden_n :] + dot_tn(late_ref[...], ref[...])


def combine_kernel(pick_ref, rows_ref, cot_ref, out_ref):
    total = dot_tn(pick_ref[...], rows_ref[...])
    out_ref[...] = (cot_ref[...].astype(F32) + total).astype(BF16)


def proj_kernel(slab_ref, act_ref, *refs):
    pieces, out_ref = refs[:-1], refs[-1]
    for j, piece in enumerate(pieces):
        out_ref[slab_ref[j]] = dot_nn(act_ref[...], piece[...]).astype(BF16)


def mixer_kernel(slab_ref, proj_ref, conv_ref, outer_ref, *refs):
    pieces, (grad_ref, back_ref) = refs[:-2], refs[-2:]
    width = pieces[0].shape[1]
    back = jnp.zeros(back_ref.shape, F32)
    for j, piece in enumerate(pieces):
        start = pl.multiple_of(slab_ref[j] * width, width)
        back = back + dot_nt(proj_ref[:, pl.ds(start, width)], piece[...])
    grad_ref[...] = (back * conv_ref[...]).astype(BF16)
    back_ref[...] = back * outer_ref[...].astype(F32)


def ring_steps(size):
    steps = [0]
    for k in range(1, size // 2):
        steps += [k, -k]
    return steps + [size // 2]


def gathered(value, axis):
    size = lax.axis_size(axis)
    pieces = [value]
    for k in ring_steps(size)[1:]:
        pieces.append(lax.ppermute(value, axis, [(i, (i + k) % size) for i in range(size)]))
    return pieces


def from_behind(value, axis, steps):
    count = lax.axis_size(axis)
    first, last = (max(0, -steps), min(count, count - steps))
    return lax.ppermute(value, axis, [(source, source + steps) for source in range(first, last)])


def shards(
    conv_outer,
    conv_inner,
    conv_input,
    conv_taps,
    out_proj,
    mixed_state,
    route_ids,
    route_weights,
    w_gate,
    w_up,
    w_down,
    cotangent,
):
    tok_count, width = mixed_state.shape
    sp_size = lax.axis_size("sp")
    z_size = lax.axis_size("z")
    slabs = 2 * z_size
    local_experts, hidden_n, features = w_gate.shape
    experts = local_experts * sp_size
    cap = 4 * tok_count // experts
    slots = experts * cap
    core, place = lax.axis_index("c"), lax.axis_index("z")
    origin = (place - jnp.array(ring_steps(z_size), jnp.int32)) % z_size
    slab_of = jnp.concatenate([2 * origin + core, 2 * origin + 1 - core]).astype(jnp.int32)
    shape = jax.ShapeDtypeStruct

    cot_pieces = gathered(cotangent, "z")

    early = cap // 8
    late_n = cap - early
    own, late_rows = experts * (cap + early), experts * late_n
    sent_rows, pick, late_pick, late_scale = pl.pallas_call(
        functools.partial(route_kernel, experts, cap, early),
        out_shape=(
            shape((own, width), BF16),
            shape((slots, tok_count), BF16),
            shape((late_rows, tok_count), BF16),
            shape((late_rows, 128), F32),
        ),
        cost_estimate=cost(2 * slots * tok_count * width, 4 * slots * width),
        name="route",
    compiler_params=grant(20),
    )(route_ids.T, route_weights.T, mixed_state, cotangent)
    recv_rows = lax.all_to_all(
        sent_rows.reshape(experts, cap + early, width), "sp", split_axis=0, concat_axis=0, tiled=True
    )
    state_all = lax.all_gather(recv_rows.reshape(own, width), TP, axis=0, tiled=False)

    half = z_size // 2 * width
    swap = [(0, 1), (1, 0)]

    def spread(pieces):
      return pl.pallas_call(
          spread_kernel,
          out_shape=shape((late_rows, half), BF16),
          cost_estimate=cost(2 * late_rows * tok_count * half, 4 * late_rows * half),
          compiler_params=grant(12),
      )(late_pick, late_scale, *pieces)

    def exchanged(part):
        got = lax.all_to_all(
            part.reshape(experts, late_n, half), "sp", split_axis=0, concat_axis=0, tiled=True
        ).reshape(late_rows, half)
        return got, lax.ppermute(got, "c", swap)

    my_low, their_low = exchanged(spread(cot_pieces[: z_size // 2]))
    my_high, their_high = exchanged(spread(cot_pieces[z_size // 2 :]))
    cots = (my_low, my_high, their_low, their_high)

    steps = 4
    whole = lambda *dims: pl.BlockSpec(dims, lambda *_: (0,) * len(dims))
    by_rows = lambda *dims: pl.BlockSpec(dims, lambda r, slab: (r, 0))
    weights = (w_gate[0], w_up[0], w_down[0])
    pre = pl.pallas_call(
        functools.partial(expert_first_kernel, cap, early),
        grid_spec=pltpu.PrefetchScalarGridSpec(
            num_scalar_prefetch=1,
            grid=(steps,),
            in_specs=[
                pl.BlockSpec((slabs // steps, own, width), lambda k, slab: (k, 0, 0)),
                *[pl.BlockSpec((late_rows, width), lambda k, slab: (0, k))] * 2,
                *[pl.BlockSpec((hidden_n, features // steps), lambda k, slab: (0, k))] * 3,
                whole(hidden_n, features),
            ],
            out_specs=whole(slots, 3 * hidden_n),
            scratch_shapes=[
                pltpu.VMEM((own, 3 * hidden_n), F32),
                pltpu.VMEM((late_rows, hidden_n), F32),
            ],
        ),
        out_shape=shape((slots, 3 * hidden_n), F32),
        cost_estimate=cost(6 * slots * hidden_n * features, 3 * slots * features),
        name="expert_first",
    compiler_params=grant(57),
    )(slab_of, state_all, my_low, their_low, *weights, w_down[0])
    partial_value, acts, late_acts = pl.pallas_call(
        functools.partial(expert_second_kernel, cap, early),
        grid_spec=pltpu.PrefetchScalarGridSpec(
            num_scalar_prefetch=1,
            grid=(steps,),
            in_specs=[
                by_rows(slots // steps, 3 * hidden_n),
                *[by_rows(late_rows // steps, half)] * 2,
                *[whole(hidden_n, features)] * 3,
            ],
            out_specs=[
                pl.BlockSpec((slabs, slots // steps, width), lambda r, slab: (0, r, 0)),
                by_rows(own // steps, 3 * hidden_n),
                by_rows(late_rows // steps, hidden_n),
            ],
            scratch_shapes=[pltpu.VMEM((2 * hidden_n, features), BF16)],
        ),
        out_shape=(
            shape((slabs, slots, width), BF16),
            shape((own, 3 * hidden_n), BF16),
            shape((late_rows, hidden_n), BF16),
        ),
        cost_estimate=cost(5 * slots * hidden_n * features, 4 * slots * features),
        name="expert_second",
        compiler_params=grant(57),
    )(slab_of, pre, my_high, their_high, *weights)

    row_back = lax.psum_scatter(partial_value, TP, scatter_dimension=0, tiled=False)

    quarter = slabs // 4

    def cot_piece(q):
        return pl.BlockSpec(
            (late_rows, width), lambda s, slab: (0, jnp.clip(s - q * quarter, 0, quarter - 1))
        )

    grad_out = pl.BlockSpec((hidden_n, width), lambda s, slab: (0, slab[s]))
    grad_gate, grad_up, grad_down = pl.pallas_call(
        weight_grad_kernel,
        grid_spec=pltpu.PrefetchScalarGridSpec(
            num_scalar_prefetch=1,
            grid=(slabs,),
            in_specs=[
                whole(own, 3 * hidden_n),
                whole(late_rows, hidden_n),
                pl.BlockSpec((1, own, width), lambda s, slab: (slab[s], 0, 0)),
                *[cot_piece(q) for q in range(4)],
            ],
            out_specs=[grad_out] * 3,
        ),
        out_shape=(shape((hidden_n, features), F32),) * 3,
        cost_estimate=cost(6 * slots * hidden_n * features, 6 * slots * features),
        name="weight_grads",
        compiler_params=grant(57),
    )(slab_of, acts, late_acts, state_all, *cots)
    row_back, grad_gate, grad_up, grad_down = lax.optimization_barrier(
        (row_back, grad_gate, grad_up, grad_down)
    )

    arrived = lax.all_to_all(
        row_back.reshape(experts, cap, width), "sp", split_axis=0, concat_axis=0, tiled=True
    ).reshape(slots, width)
    grad_mixed = pl.pallas_call(
        combine_kernel,
        out_shape=shape((tok_count, width), BF16),
        cost_estimate=cost(2 * slots * tok_count * width, 4 * slots * width),
        name="combine",
        compiler_params=grant(16),
    )(pick, arrived, cotangent)
    near = gathered(grad_mixed, "z")
    full_back = near + [lax.ppermute(piece, "c", swap) for piece in near]

    taps_count = conv_taps.shape[0]
    rim_width = taps_count - 1
    channels = conv_inner.shape[0]
    head_block = from_behind(
        jnp.stack([conv_inner[:, tok_count - rim_width :], conv_input[:, tok_count - rim_width :]]),
        "sp",
        1,
    )
    inner_ext = jnp.concatenate([head_block[0], conv_inner], axis=1).astype(F32)
    input_ext = jnp.concatenate([head_block[1], conv_input], axis=1).astype(F32)
    inner_prod = inner_ext * input_ext
    conv_out = jnp.zeros((channels, tok_count), F32)
    for offset in range(taps_count):
        conv_out = (
            conv_out + conv_taps[offset][:, None] * inner_prod[:, offset : offset + tok_count]
        )
    mixer_act = (conv_outer.astype(F32) * conv_out).astype(BF16)

    vmem, smem = pl.BlockSpec(memory_space=pltpu.VMEM), pl.BlockSpec(memory_space=pltpu.SMEM)
    proj_term = pl.pallas_call(
        proj_kernel,
        in_specs=[smem] + [vmem] * (1 + slabs),
        out_shape=shape((slabs, channels, width), BF16),
        cost_estimate=cost(2 * channels * tok_count * features, 4 * tok_count * features),
        name="proj",
        compiler_params=grant(14),
    )(slab_of, mixer_act, *full_back)
    landed = lax.all_to_all(proj_term, "sp", split_axis=0, concat_axis=0, tiled=True)
    grad_proj = jnp.sum(landed.astype(F32), axis=0)
    grad_outer, back_conv = pl.pallas_call(
        mixer_kernel,
        in_specs=[smem] + [vmem] * (3 + slabs),
        out_shape=(shape((channels, tok_count), BF16), shape((channels, tok_count), F32)),
        cost_estimate=cost(2 * channels * tok_count * features, 4 * tok_count * features),
        name="mixer",
        compiler_params=grant(14),
    )(slab_of, out_proj, conv_out, conv_outer, *full_back)
    tail_back = from_behind(back_conv[:, :rim_width], "sp", -1)
    back_ext = jnp.concatenate([back_conv, tail_back], axis=1)
    back_prod = jnp.zeros_like(back_conv)
    for offset in range(taps_count):
        shift_by = rim_width - offset
        back_prod = (
            back_prod + conv_taps[offset][:, None] * back_ext[:, shift_by : shift_by + tok_count]
        )
    grad_inner = (back_prod * conv_input.astype(F32)).astype(BF16)
    grad_input = (back_prod * conv_inner.astype(F32)).astype(BF16)
    return (
        grad_gate[None],
        grad_up[None],
        grad_down[None],
        grad_mixed,
        grad_proj,
        grad_outer,
        grad_inner,
        grad_input,
    )


def solution(mesh):
    torus = Mesh(mesh.devices.reshape(mesh.shape["sp"], mesh.shape["tp"] // 2, 2), ("sp", "z", "c"))

    return jax.shard_map(
        shards,
        mesh=torus,
        in_specs=(
            P(TP, "sp"),
            P(TP, "sp"),
            P(TP, "sp"),
            P(None, TP),
            P(TP, None),
            P("sp", TP),
            P("sp", None),
            P("sp", None),
            P("sp", TP, None),
            P("sp", TP, None),
            P("sp", TP, None),
            P("sp", TP),
        ),
        out_specs=(
            P("sp", TP, None),
            P("sp", TP, None),
            P("sp", TP, None),
            P("sp", TP),
            P(TP, "sp"),
            P(TP, "sp"),
            P(TP, "sp"),
            P(TP, "sp"),
        ),
        check_vma=False,
    )
```

```python
import functools

import jax
import jax.numpy as jnp
from jax import lax
from jax.experimental import pallas as pl
from jax.experimental.pallas import tpu as pltpu
from jax.sharding import Mesh
from jax.sharding import PartitionSpec as P


TP = ("z", "c")
BF16 = jnp.bfloat16
F32 = jnp.float32


def dot_nn(a, b):
    return lax.dot_general(a, b, (((1,), (0,)), ((), ())), preferred_element_type=F32)


def dot_nt(a, b):
    return lax.dot_general(a, b, (((1,), (1,)), ((), ())), preferred_element_type=F32)


def dot_tn(a, b):
    return lax.dot_general(a, b, (((0,), (0,)), ((), ())), preferred_element_type=F32)


def grant(mib):
    return pltpu.CompilerParams(vmem_limit_bytes=mib << 20)


def cost(flops, nbytes):
    return pl.CostEstimate(flops=int(flops), bytes_accessed=int(nbytes), transcendentals=0)


def route_kernel(experts, cap, ids_ref, wts_ref, state_ref, sent_ref, pick_ref, scale_ref):
    tokens = ids_ref.shape[1]
    first, second = ids_ref[0:1, :], ids_ref[1:2, :]
    expert = lax.broadcasted_iota(jnp.int32, (experts, tokens), 0)
    is_first, is_second = first == expert, second == expert
    named = jnp.logical_or(is_first, is_second)
    before = lax.broadcasted_iota(jnp.int32, (tokens, tokens), 0) < lax.broadcasted_iota(
        jnp.int32, (tokens, tokens), 1
    )
    earlier = dot_nn(named.astype(F32).astype(BF16), before.astype(F32).astype(BF16))
    slot = jnp.where(named, earlier.astype(jnp.int32), -1)
    weight = jnp.where(is_first, wts_ref[0:1, :], jnp.where(is_second, wts_ref[1:2, :], 0.0))
    place = lax.broadcasted_iota(jnp.int32, (cap, tokens), 0)
    for e in range(experts):
        hit = slot[e : e + 1, :] == place
        pick_ref[e * cap : (e + 1) * cap, :] = hit.astype(F32).astype(BF16)
        taken = jnp.sum(jnp.where(hit, weight[e : e + 1, :], 0.0), axis=1, keepdims=True)
        scale_ref[e * cap : (e + 1) * cap, :] = jnp.broadcast_to(taken, (cap, 128))
    sent_ref[...] = dot_nn(pick_ref[...], state_ref[...]).astype(BF16)


def spread_kernel(late_ref, scale_ref, *refs):
    pieces, out_ref = refs[:-1], refs[-1]
    width = pieces[0].shape[1]
    scale = scale_ref[:, 0:1]
    for j, piece in enumerate(pieces):
        rows = (dot_nn(late_ref[...], piece[...]) * scale).astype(BF16)
        out_ref[:, j * width : (j + 1) * width] = rows


def down_columns(slab_ref, base, wd_ref, count, width):
    pieces = [
        wd_ref[:, pl.ds(pl.multiple_of(slab_ref[base + j] * width, width), width)]
        for j in range(count)
    ]
    return jnp.concatenate(pieces, axis=1)


def expert_first_kernel(
    slab_ref, state_ref, mine_ref, their_ref, wg_ref, wu_ref, wd_ref, pre_ref
):
    slabs, width = state_ref.shape[0], state_ref.shape[2]
    hidden_n = wd_ref.shape[0]
    step, steps = pl.program_id(0), pl.num_programs(0)
    rows = jnp.concatenate([state_ref[s] for s in range(slabs)], axis=1)
    both = dot_nt(rows, jnp.concatenate([wg_ref[...], wu_ref[...]], axis=0))

    def down(base):
        at = pl.multiple_of(slab_ref[base + step] * width, width)
        return wd_ref[:, pl.ds(at, width)]

    cots = jnp.concatenate([mine_ref[...], their_ref[...]], axis=1)
    back = dot_nt(cots, jnp.concatenate([down(0), down(2 * steps)], axis=1))

    @pl.when(step == 0)
    def _():
        pre_ref[:, : 2 * hidden_n] = both
        pre_ref[:, 2 * hidden_n :] = back

    @pl.when(step > 0)
    def _():
        pre_ref[:, : 2 * hidden_n] += both
        pre_ref[:, 2 * hidden_n :] += back


def expert_second_kernel(
    slab_ref, pre_ref, mine_ref, their_ref, wg_ref, wu_ref, wd_ref, part_ref, act_ref, w_ref
):
    slabs, width = part_ref.shape[0], part_ref.shape[2]
    hidden_n = wd_ref.shape[0]

    @pl.when(pl.program_id(0) == 0)
    def _():
        w_ref[:hidden_n] = wg_ref[...]
        w_ref[hidden_n:] = wu_ref[...]

    per = mine_ref.shape[1] // width
    gate_pre, up_pre = pre_ref[:, :hidden_n], pre_ref[:, hidden_n : 2 * hidden_n]
    back_hidden = pre_ref[:, 2 * hidden_n :]
    back_hidden = back_hidden + dot_nt(mine_ref[...], down_columns(slab_ref, per, wd_ref, per, width))
    back_hidden = back_hidden + dot_nt(
        their_ref[...], down_columns(slab_ref, 3 * per, wd_ref, per, width)
    )
    sig_gate = jax.nn.sigmoid(gate_pre)
    silu_gate = gate_pre * sig_gate
    hidden = (silu_gate * up_pre).astype(BF16)
    back_gate = (back_hidden * up_pre * sig_gate * (1.0 + gate_pre * (1.0 - sig_gate))).astype(BF16)
    back_up = (back_hidden * silu_gate).astype(BF16)
    back = jnp.concatenate([back_gate, back_up], axis=1)
    for s in range(slabs):
        part_ref[s] = dot_nn(back, w_ref[:, s * width : (s + 1) * width]).astype(BF16)
    act_ref[:, : 2 * hidden_n] = back
    act_ref[:, 2 * hidden_n :] = hidden


def weight_grad_kernel(
    slab_ref, act_ref, state_ref, ml_ref, mh_ref, tl_ref, th_ref, gg_ref, gu_ref, gd_ref
):
    hidden_n = gg_ref.shape[0]
    step, per = pl.program_id(0), pl.num_programs(0) // 4
    both = dot_tn(act_ref[:, : 2 * hidden_n], state_ref[0])
    gg_ref[...] = both[:hidden_n]
    gu_ref[...] = both[hidden_n:]
    for q, ref in enumerate((ml_ref, mh_ref, tl_ref, th_ref)):

        @pl.when(step // per == q)
        def _(ref=ref):
            gd_ref[...] = dot_tn(act_ref[:, 2 * hidden_n :], ref[...])


def combine_kernel(pick_ref, rows_ref, cot_ref, out_ref):
    total = dot_tn(pick_ref[...], rows_ref[...])
    out_ref[...] = (cot_ref[...].astype(F32) + total).astype(BF16)


def proj_kernel(slab_ref, act_ref, *refs):
    pieces, out_ref = refs[:-1], refs[-1]
    for j, piece in enumerate(pieces):
        out_ref[slab_ref[j]] = dot_nn(act_ref[...], piece[...]).astype(BF16)


def mixer_kernel(slab_ref, proj_ref, conv_ref, outer_ref, *refs):
    pieces, (grad_ref, back_ref) = refs[:-2], refs[-2:]
    width = pieces[0].shape[1]
    back = jnp.zeros(back_ref.shape, F32)
    for j, piece in enumerate(pieces):
        start = pl.multiple_of(slab_ref[j] * width, width)
        back = back + dot_nt(proj_ref[:, pl.ds(start, width)], piece[...])
    grad_ref[...] = (back * conv_ref[...]).astype(BF16)
    back_ref[...] = back * outer_ref[...].astype(F32)


def ring_steps(size):
    steps = [0]
    for k in range(1, size // 2):
        steps += [k, -k]
    return steps + [size // 2]


def gathered(value, axis):
    size = lax.axis_size(axis)
    pieces = [value]
    for k in ring_steps(size)[1:]:
        pieces.append(lax.ppermute(value, axis, [(i, (i + k) % size) for i in range(size)]))
    return pieces


def from_behind(value, axis, steps):
    count = lax.axis_size(axis)
    first, last = (max(0, -steps), min(count, count - steps))
    return lax.ppermute(value, axis, [(source, source + steps) for source in range(first, last)])


def shards(
    conv_outer,
    conv_inner,
    conv_input,
    conv_taps,
    out_proj,
    mixed_state,
    route_ids,
    route_weights,
    w_gate,
    w_up,
    w_down,
    cotangent,
):
    tok_count, width = mixed_state.shape
    sp_size = lax.axis_size("sp")
    z_size = lax.axis_size("z")
    slabs = 2 * z_size
    local_experts, hidden_n, features = w_gate.shape
    experts = local_experts * sp_size
    cap = 4 * tok_count // experts
    slots = experts * cap
    core, place = lax.axis_index("c"), lax.axis_index("z")
    origin = (place - jnp.array(ring_steps(z_size), jnp.int32)) % z_size
    slab_of = jnp.concatenate([2 * origin + core, 2 * origin + 1 - core]).astype(jnp.int32)
    shape = jax.ShapeDtypeStruct

    cot_pieces = gathered(cotangent, "z")

    sent_rows, pick, scale = pl.pallas_call(
        functools.partial(route_kernel, experts, cap),
        out_shape=(
            shape((slots, width), BF16),
            shape((slots, tok_count), BF16),
            shape((slots, 128), F32),
        ),
        cost_estimate=cost(2 * slots * tok_count * width, 4 * slots * width),
        name="route",
    )(route_ids.T, route_weights.T, mixed_state)
    recv_rows = lax.all_to_all(
        sent_rows.reshape(experts, cap, width), "sp", split_axis=0, concat_axis=0, tiled=True
    )
    state_all = lax.all_gather(recv_rows.reshape(slots, width), TP, axis=0, tiled=False)

    half = z_size // 2 * width
    swap = [(0, 1), (1, 0)]

    def spread(pieces):
        return pl.pallas_call(
            spread_kernel,
            out_shape=shape((slots, half), BF16),
            cost_estimate=cost(2 * slots * tok_count * half, 4 * slots * half),
            compiler_params=grant(16),
        )(pick, scale, *pieces)

    def exchanged(part):
        got = lax.all_to_all(
            part.reshape(experts, cap, half), "sp", split_axis=0, concat_axis=0, tiled=True
        ).reshape(slots, half)
        return got, lax.ppermute(got, "c", swap)

    my_low, their_low = exchanged(spread(cot_pieces[: z_size // 2]))
    my_high, their_high = exchanged(spread(cot_pieces[z_size // 2 :]))
    cots = (my_low, my_high, their_low, their_high)

    steps = 4
    whole = lambda *dims: pl.BlockSpec(dims, lambda *_: (0,) * len(dims))
    by_rows = lambda *dims: pl.BlockSpec(dims, lambda r, slab: (r, 0))
    weights = (w_gate[0], w_up[0], w_down[0])
    pre = pl.pallas_call(
        expert_first_kernel,
        grid_spec=pltpu.PrefetchScalarGridSpec(
            num_scalar_prefetch=1,
            grid=(steps,),
            in_specs=[
                pl.BlockSpec((slabs // steps, slots, width), lambda k, slab: (k, 0, 0)),
                *[pl.BlockSpec((slots, width), lambda k, slab: (0, k))] * 2,
                *[pl.BlockSpec((hidden_n, features // steps), lambda k, slab: (0, k))] * 2,
                whole(hidden_n, features),
            ],
            out_specs=whole(slots, 3 * hidden_n),
        ),
        out_shape=shape((slots, 3 * hidden_n), F32),
        cost_estimate=cost(5 * slots * hidden_n * features, 3 * slots * features),
        name="expert_first",
    )(slab_of, state_all, my_low, their_low, *weights)
    partial_value, acts = pl.pallas_call(
        expert_second_kernel,
        grid_spec=pltpu.PrefetchScalarGridSpec(
            num_scalar_prefetch=1,
            grid=(steps,),
            in_specs=[
                by_rows(slots // steps, 3 * hidden_n),
                *[by_rows(slots // steps, half)] * 2,
                *[whole(hidden_n, features)] * 3,
            ],
            out_specs=[
                pl.BlockSpec((slabs, slots // steps, width), lambda r, slab: (0, r, 0)),
                by_rows(slots // steps, 3 * hidden_n),
            ],
            scratch_shapes=[pltpu.VMEM((2 * hidden_n, features), BF16)],
        ),
        out_shape=(shape((slabs, slots, width), BF16), shape((slots, 3 * hidden_n), BF16)),
        cost_estimate=cost(5 * slots * hidden_n * features, 4 * slots * features),
        name="expert_second",
    )(slab_of, pre, my_high, their_high, *weights)

    row_back = lax.psum_scatter(partial_value, TP, scatter_dimension=0, tiled=False)

    quarter = slabs // 4

    def cot_piece(q):
        return pl.BlockSpec(
            (slots, width), lambda s, slab: (0, jnp.clip(s - q * quarter, 0, quarter - 1))
        )

    grad_out = pl.BlockSpec((hidden_n, width), lambda s, slab: (0, slab[s]))
    grad_gate, grad_up, grad_down = pl.pallas_call(
        weight_grad_kernel,
        grid_spec=pltpu.PrefetchScalarGridSpec(
            num_scalar_prefetch=1,
            grid=(slabs,),
            in_specs=[
                whole(slots, 3 * hidden_n),
                pl.BlockSpec((1, slots, width), lambda s, slab: (slab[s], 0, 0)),
                *[cot_piece(q) for q in range(4)],
            ],
            out_specs=[grad_out] * 3,
        ),
        out_shape=(shape((hidden_n, features), F32),) * 3,
        cost_estimate=cost(6 * slots * hidden_n * features, 6 * slots * features),
        name="weight_grads",
    )(slab_of, acts, state_all, *cots)
    row_back, grad_gate, grad_up, grad_down = lax.optimization_barrier(
        (row_back, grad_gate, grad_up, grad_down)
    )

    arrived = lax.all_to_all(
        row_back.reshape(experts, cap, width), "sp", split_axis=0, concat_axis=0, tiled=True
    ).reshape(slots, width)
    grad_mixed = pl.pallas_call(
        combine_kernel,
        out_shape=shape((tok_count, width), BF16),
        cost_estimate=cost(2 * slots * tok_count * width, 4 * slots * width),
        name="combine",
        compiler_params=grant(16),
    )(pick, arrived, cotangent)
    near = gathered(grad_mixed, "z")
    full_back = near + [lax.ppermute(piece, "c", swap) for piece in near]

    taps_count = conv_taps.shape[0]
    rim_width = taps_count - 1
    channels = conv_inner.shape[0]
    head_block = from_behind(
        jnp.stack([conv_inner[:, tok_count - rim_width :], conv_input[:, tok_count - rim_width :]]),
        "sp",
        1,
    )
    inner_ext = jnp.concatenate([head_block[0], conv_inner], axis=1).astype(F32)
    input_ext = jnp.concatenate([head_block[1], conv_input], axis=1).astype(F32)
    inner_prod = inner_ext * input_ext
    conv_out = jnp.zeros((channels, tok_count), F32)
    for offset in range(taps_count):
        conv_out = (
            conv_out + conv_taps[offset][:, None] * inner_prod[:, offset : offset + tok_count]
        )
    mixer_act = (conv_outer.astype(F32) * conv_out).astype(BF16)

    vmem, smem = pl.BlockSpec(memory_space=pltpu.VMEM), pl.BlockSpec(memory_space=pltpu.SMEM)
    proj_term = pl.pallas_call(
        proj_kernel,
        in_specs=[smem] + [vmem] * (1 + slabs),
        out_shape=shape((slabs, channels, width), BF16),
        cost_estimate=cost(2 * channels * tok_count * features, 4 * tok_count * features),
        name="proj",
        compiler_params=grant(14),
    )(slab_of, mixer_act, *full_back)
    landed = lax.all_to_all(proj_term, "sp", split_axis=0, concat_axis=0, tiled=True)
    grad_proj = jnp.sum(landed.astype(F32), axis=0)
    grad_outer, back_conv = pl.pallas_call(
        mixer_kernel,
        in_specs=[smem] + [vmem] * (3 + slabs),
        out_shape=(shape((channels, tok_count), BF16), shape((channels, tok_count), F32)),
        cost_estimate=cost(2 * channels * tok_count * features, 4 * tok_count * features),
        name="mixer",
        compiler_params=grant(14),
    )(slab_of, out_proj, conv_out, conv_outer, *full_back)
    tail_back = from_behind(back_conv[:, :rim_width], "sp", -1)
    back_ext = jnp.concatenate([back_conv, tail_back], axis=1)
    back_prod = jnp.zeros_like(back_conv)
    for offset in range(taps_count):
        shift_by = rim_width - offset
        back_prod = (
            back_prod + conv_taps[offset][:, None] * back_ext[:, shift_by : shift_by + tok_count]
        )
    grad_inner = (back_prod * conv_input.astype(F32)).astype(BF16)
    grad_input = (back_prod * conv_inner.astype(F32)).astype(BF16)
    return (
        grad_gate[None],
        grad_up[None],
        grad_down[None],
        grad_mixed,
        grad_proj,
        grad_outer,
        grad_inner,
        grad_input,
    )


def solution(mesh):
    torus = Mesh(mesh.devices.reshape(mesh.shape["sp"], mesh.shape["tp"] // 2, 2), ("sp", "z", "c"))

    return jax.shard_map(
        shards,
        mesh=torus,
        in_specs=(
            P(TP, "sp"),
            P(TP, "sp"),
            P(TP, "sp"),
            P(None, TP),
            P(TP, None),
            P("sp", TP),
            P("sp", None),
            P("sp", None),
            P("sp", TP, None),
            P("sp", TP, None),
            P("sp", TP, None),
            P("sp", TP),
        ),
        out_specs=(
            P("sp", TP, None),
            P("sp", TP, None),
            P("sp", TP, None),
            P("sp", TP),
            P(TP, "sp"),
            P(TP, "sp"),
            P(TP, "sp"),
            P(TP, "sp"),
        ),
        check_vma=False,
    )
```

```python
import functools

import jax
import jax.numpy as jnp
from jax import lax
from jax.experimental import pallas as pl
from jax.experimental.pallas import tpu as pltpu
from jax.sharding import Mesh
from jax.sharding import PartitionSpec as P


TP = ("z", "c")
BF16 = jnp.bfloat16
F32 = jnp.float32


def dot_nn(a, b):
    return lax.dot_general(a, b, (((1,), (0,)), ((), ())), preferred_element_type=F32)


def dot_nt(a, b):
    return lax.dot_general(a, b, (((1,), (1,)), ((), ())), preferred_element_type=F32)


def dot_tn(a, b):
    return lax.dot_general(a, b, (((0,), (0,)), ((), ())), preferred_element_type=F32)


def grant(mib):
    return pltpu.CompilerParams(vmem_limit_bytes=mib << 20)


def cost(flops, nbytes):
    return pl.CostEstimate(flops=int(flops), bytes_accessed=int(nbytes), transcendentals=0)


def route_kernel(experts, cap, ids_ref, wts_ref, state_ref, sent_ref, pick_ref, scale_ref):
    tokens = ids_ref.shape[1]
    first, second = ids_ref[0:1, :], ids_ref[1:2, :]
    expert = lax.broadcasted_iota(jnp.int32, (experts, tokens), 0)
    is_first, is_second = first == expert, second == expert
    named = jnp.logical_or(is_first, is_second)
    before = lax.broadcasted_iota(jnp.int32, (tokens, tokens), 0) < lax.broadcasted_iota(
        jnp.int32, (tokens, tokens), 1
    )
    earlier = dot_nn(named.astype(F32).astype(BF16), before.astype(F32).astype(BF16))
    slot = jnp.where(named, earlier.astype(jnp.int32), -1)
    weight = jnp.where(is_first, wts_ref[0:1, :], jnp.where(is_second, wts_ref[1:2, :], 0.0))
    place = lax.broadcasted_iota(jnp.int32, (cap, tokens), 0)
    for e in range(experts):
        hit = slot[e : e + 1, :] == place
        pick_ref[e * cap : (e + 1) * cap, :] = hit.astype(F32).astype(BF16)
        taken = jnp.sum(jnp.where(hit, weight[e : e + 1, :], 0.0), axis=1, keepdims=True)
        scale_ref[e * cap : (e + 1) * cap, :] = jnp.broadcast_to(taken, (cap, 128))
    sent_ref[...] = dot_nn(pick_ref[...], state_ref[...]).astype(BF16)


def spread_kernel(pick_ref, scale_ref, *refs):
    pieces, out_ref = refs[:-1], refs[-1]
    width = pieces[0].shape[1]
    scale = scale_ref[:, 0:1]
    for j, piece in enumerate(pieces):
        rows = (dot_nn(pick_ref[...], piece[...]) * scale).astype(BF16)
        out_ref[:, j * width : (j + 1) * width] = rows


def expert_kernel(
    slab_ref, state_ref, ml_ref, mh_ref, tl_ref, th_ref, wg_ref, wu_ref, wd_ref, part_ref, act_ref, wgu_ref
):
    slabs, width = state_ref.shape[0], state_ref.shape[2]
    hidden_n = wd_ref.shape[0]

    @pl.when(pl.program_id(0) == 0)
    def _():
        wgu_ref[:hidden_n] = wg_ref[...]
        wgu_ref[hidden_n:] = wu_ref[...]

    rows = jnp.concatenate([state_ref[s] for s in range(slabs)], axis=1)
    pre = dot_nt(rows, wgu_ref[...])
    gate_pre, up_pre = pre[:, :hidden_n], pre[:, hidden_n:]
    back_hidden = jnp.zeros(gate_pre.shape, F32)
    per = ml_ref.shape[1] // width
    for q, ref in enumerate((ml_ref, mh_ref, tl_ref, th_ref)):
        pieces = [
            wd_ref[:, pl.ds(pl.multiple_of(slab_ref[q * per + j] * width, width), width)]
            for j in range(per)
        ]
        back_hidden = back_hidden + dot_nt(ref[...], jnp.concatenate(pieces, axis=1))
    sig_gate = jax.nn.sigmoid(gate_pre)
    silu_gate = gate_pre * sig_gate
    hidden = (silu_gate * up_pre).astype(BF16)
    back_gate = (back_hidden * up_pre * sig_gate * (1.0 + gate_pre * (1.0 - sig_gate))).astype(BF16)
    back_up = (back_hidden * silu_gate).astype(BF16)
    back = jnp.concatenate([back_gate, back_up], axis=1)
    act_ref[:, : 2 * hidden_n] = back
    act_ref[:, 2 * hidden_n :] = hidden
    for s in range(slabs):
        part_ref[s] = dot_nn(back, wgu_ref[:, s * width : (s + 1) * width]).astype(BF16)


def weight_grad_kernel(slab_ref, act_ref, state_ref, ml_ref, mh_ref, tl_ref, th_ref, gg_ref, gu_ref, gd_ref):
    hidden_n = gg_ref.shape[0]
    step, per = pl.program_id(0), pl.num_programs(0) // 4
    both = dot_tn(act_ref[:, : 2 * hidden_n], state_ref[0])
    gg_ref[...] = both[:hidden_n]
    gu_ref[...] = both[hidden_n:]
    for q, ref in enumerate((ml_ref, mh_ref, tl_ref, th_ref)):

        @pl.when(step // per == q)
        def _(ref=ref):
            gd_ref[...] = dot_tn(act_ref[:, 2 * hidden_n :], ref[...])


def combine_kernel(pick_ref, rows_ref, cot_ref, out_ref):
    total = dot_tn(pick_ref[...], rows_ref[...])
    out_ref[...] = (cot_ref[...].astype(F32) + total).astype(BF16)


def proj_kernel(slab_ref, act_ref, *refs):
    pieces, out_ref = refs[:-1], refs[-1]
    for j, piece in enumerate(pieces):
        out_ref[slab_ref[j]] = dot_nn(act_ref[...], piece[...]).astype(BF16)


def mixer_kernel(slab_ref, proj_ref, conv_ref, outer_ref, *refs):
    pieces, (grad_ref, back_ref) = refs[:-2], refs[-2:]
    width = pieces[0].shape[1]
    back = jnp.zeros(back_ref.shape, F32)
    for j, piece in enumerate(pieces):
        start = pl.multiple_of(slab_ref[j] * width, width)
        back = back + dot_nt(proj_ref[:, pl.ds(start, width)], piece[...])
    grad_ref[...] = (back * conv_ref[...]).astype(BF16)
    back_ref[...] = back * outer_ref[...].astype(F32)


def ring_steps(size):
    steps = [0]
    for k in range(1, size // 2):
        steps += [k, -k]
    return steps + [size // 2]


def gathered(value, axis):
    size = lax.axis_size(axis)
    pieces = [value]
    for k in ring_steps(size)[1:]:
        pieces.append(lax.ppermute(value, axis, [(i, (i + k) % size) for i in range(size)]))
    return pieces


def from_behind(value, axis, steps):
    count = lax.axis_size(axis)
    first, last = (max(0, -steps), min(count, count - steps))
    return lax.ppermute(value, axis, [(source, source + steps) for source in range(first, last)])


def shards(
    conv_outer,
    conv_inner,
    conv_input,
    conv_taps,
    out_proj,
    mixed_state,
    route_ids,
    route_weights,
    w_gate,
    w_up,
    w_down,
    cotangent,
):
    tok_count, width = mixed_state.shape
    sp_size = lax.axis_size("sp")
    z_size = lax.axis_size("z")
    slabs = 2 * z_size
    local_experts, hidden_n, features = w_gate.shape
    experts = local_experts * sp_size
    cap = 4 * tok_count // experts
    slots = experts * cap
    core, place = lax.axis_index("c"), lax.axis_index("z")
    origin = (place - jnp.array(ring_steps(z_size), jnp.int32)) % z_size
    slab_of = jnp.concatenate([2 * origin + core, 2 * origin + 1 - core]).astype(jnp.int32)
    shape = jax.ShapeDtypeStruct

    cot_pieces = gathered(cotangent, "z")

    sent_state, pick, scale = pl.pallas_call(
        functools.partial(route_kernel, experts, cap),
        out_shape=(
            shape((slots, width), BF16),
            shape((slots, tok_count), BF16),
            shape((slots, 128), F32),
        ),
        cost_estimate=cost(2 * slots * tok_count * width, 4 * slots * width),
        name="route",
    )(route_ids.T, route_weights.T, mixed_state)
    recv_state = lax.all_to_all(
        sent_state.reshape(experts, cap, width), "sp", split_axis=0, concat_axis=0, tiled=True
    )
    state_all = lax.all_gather(recv_state.reshape(slots, width), TP, axis=0, tiled=False)

    half = z_size // 2 * width
    swap = [(0, 1), (1, 0)]

    def spread(pieces):
        return pl.pallas_call(
            spread_kernel,
            out_shape=shape((slots, half), BF16),
            cost_estimate=cost(2 * slots * tok_count * half, 4 * slots * half),
        )(pick, scale, *pieces)

    def exchanged(part):
        got = lax.all_to_all(
            part.reshape(experts, cap, half), "sp", split_axis=0, concat_axis=0, tiled=True
        ).reshape(slots, half)
        return got, lax.ppermute(got, "c", swap)

    my_low, their_low = exchanged(spread(cot_pieces[: z_size // 2]))
    my_high, their_high = exchanged(spread(cot_pieces[z_size // 2 :]))
    cots = (my_low, my_high, their_low, their_high)

    block = 256
    whole = lambda *dims: pl.BlockSpec(dims, lambda *_: (0,) * len(dims))
    cot_rows = pl.BlockSpec((block, half), lambda r, core: (r, 0))
    partial_value, acts = pl.pallas_call(
        expert_kernel,
        grid_spec=pltpu.PrefetchScalarGridSpec(
            num_scalar_prefetch=1,
            grid=(slots // block,),
            in_specs=[
                pl.BlockSpec((slabs, block, width), lambda r, core: (0, r, 0)),
                *[cot_rows] * 4,
                *[whole(hidden_n, features)] * 3,
            ],
            out_specs=[
                pl.BlockSpec((slabs, block, width), lambda r, core: (0, r, 0)),
                pl.BlockSpec((block, 3 * hidden_n), lambda r, core: (r, 0)),
            ],
            scratch_shapes=[pltpu.VMEM((2 * hidden_n, features), BF16)],
        ),
        out_shape=(shape((slabs, slots, width), BF16), shape((slots, 3 * hidden_n), BF16)),
        cost_estimate=cost(10 * slots * hidden_n * features, 6 * slots * features),
        name="expert",
    )(slab_of, state_all, *cots, w_gate[0], w_up[0], w_down[0])

    row_back = lax.psum_scatter(partial_value, TP, scatter_dimension=0, tiled=False)

    quarter = slabs // 4

    def cot_piece(q):
        return pl.BlockSpec(
            (slots, width), lambda s, core: (0, jnp.clip(s - q * quarter, 0, quarter - 1))
        )

    grad_out = pl.BlockSpec((hidden_n, width), lambda s, slab: (0, slab[s]))
    grad_gate, grad_up, grad_down = pl.pallas_call(
        weight_grad_kernel,
        grid_spec=pltpu.PrefetchScalarGridSpec(
            num_scalar_prefetch=1,
            grid=(slabs,),
            in_specs=[
                whole(slots, 3 * hidden_n),
                pl.BlockSpec((1, slots, width), lambda s, slab: (slab[s], 0, 0)),
                *[cot_piece(q) for q in range(4)],
            ],
            out_specs=[grad_out] * 3,
        ),
        out_shape=(shape((hidden_n, features), F32),) * 3,
        cost_estimate=cost(6 * slots * hidden_n * features, 6 * slots * features),
        name="weight_grads",
    )(slab_of, acts, state_all, *cots)
    row_back, grad_gate, grad_up, grad_down = lax.optimization_barrier(
        (row_back, grad_gate, grad_up, grad_down)
    )

    arrived = lax.all_to_all(
        row_back.reshape(experts, cap, width), "sp", split_axis=0, concat_axis=0, tiled=True
    ).reshape(slots, width)
    grad_mixed = pl.pallas_call(
        combine_kernel,
        out_shape=shape((tok_count, width), BF16),
        cost_estimate=cost(2 * slots * tok_count * width, 4 * slots * width),
        name="combine",
        compiler_params=grant(16),
    )(pick, arrived, cotangent)
    near = gathered(grad_mixed, "z")
    full_back = near + [lax.ppermute(piece, "c", swap) for piece in near]

    taps_count = conv_taps.shape[0]
    rim_width = taps_count - 1
    channels = conv_inner.shape[0]
    head_block = from_behind(
        jnp.stack([conv_inner[:, tok_count - rim_width :], conv_input[:, tok_count - rim_width :]]),
        "sp",
        1,
    )
    inner_ext = jnp.concatenate([head_block[0], conv_inner], axis=1).astype(F32)
    input_ext = jnp.concatenate([head_block[1], conv_input], axis=1).astype(F32)
    inner_prod = inner_ext * input_ext
    conv_out = jnp.zeros((channels, tok_count), F32)
    for offset in range(taps_count):
        conv_out = (
            conv_out + conv_taps[offset][:, None] * inner_prod[:, offset : offset + tok_count]
        )
    mixer_act = (conv_outer.astype(F32) * conv_out).astype(BF16)

    vmem, smem = pl.BlockSpec(memory_space=pltpu.VMEM), pl.BlockSpec(memory_space=pltpu.SMEM)
    proj_term = pl.pallas_call(
        proj_kernel,
        in_specs=[smem] + [vmem] * (1 + slabs),
        out_shape=shape((slabs, channels, width), BF16),
        cost_estimate=cost(2 * channels * tok_count * features, 4 * tok_count * features),
        name="proj",
    )(slab_of, mixer_act, *full_back)
    landed = lax.all_to_all(proj_term, "sp", split_axis=0, concat_axis=0, tiled=True)
    grad_proj = jnp.sum(landed.astype(F32), axis=0)
    grad_outer, back_conv = pl.pallas_call(
        mixer_kernel,
        in_specs=[smem] + [vmem] * (3 + slabs),
        out_shape=(shape((channels, tok_count), BF16), shape((channels, tok_count), F32)),
        cost_estimate=cost(2 * channels * tok_count * features, 4 * tok_count * features),
        name="mixer",
    )(slab_of, out_proj, conv_out, conv_outer, *full_back)
    tail_back = from_behind(back_conv[:, :rim_width], "sp", -1)
    back_ext = jnp.concatenate([back_conv, tail_back], axis=1)
    back_prod = jnp.zeros_like(back_conv)
    for offset in range(taps_count):
        shift_by = rim_width - offset
        back_prod = (
            back_prod + conv_taps[offset][:, None] * back_ext[:, shift_by : shift_by + tok_count]
        )
    grad_inner = (back_prod * conv_input.astype(F32)).astype(BF16)
    grad_input = (back_prod * conv_inner.astype(F32)).astype(BF16)
    return (
        grad_gate[None],
        grad_up[None],
        grad_down[None],
        grad_mixed,
        grad_proj,
        grad_outer,
        grad_inner,
        grad_input,
    )


def solution(mesh):
    torus = Mesh(mesh.devices.reshape(mesh.shape["sp"], mesh.shape["tp"] // 2, 2), ("sp", "z", "c"))

    return jax.shard_map(
        shards,
        mesh=torus,
        in_specs=(
            P(TP, "sp"),
            P(TP, "sp"),
            P(TP, "sp"),
            P(None, TP),
            P(TP, None),
            P("sp", TP),
            P("sp", None),
            P("sp", None),
            P("sp", TP, None),
            P("sp", TP, None),
            P("sp", TP, None),
            P("sp", TP),
        ),
        out_specs=(
            P("sp", TP, None),
            P("sp", TP, None),
            P("sp", TP, None),
            P("sp", TP),
            P(TP, "sp"),
            P(TP, "sp"),
            P(TP, "sp"),
            P(TP, "sp"),
        ),
        check_vma=False,
    )
```

```python
import functools

import jax
import jax.numpy as jnp
from jax import lax
from jax.experimental import pallas as pl
from jax.experimental.pallas import tpu as pltpu
from jax.sharding import Mesh
from jax.sharding import PartitionSpec as P


TP = ("z", "c")
BF16 = jnp.bfloat16
F32 = jnp.float32


def dot_nn(a, b):
    return lax.dot_general(a, b, (((1,), (0,)), ((), ())), preferred_element_type=F32)


def dot_nt(a, b):
    return lax.dot_general(a, b, (((1,), (1,)), ((), ())), preferred_element_type=F32)


def dot_tn(a, b):
    return lax.dot_general(a, b, (((0,), (0,)), ((), ())), preferred_element_type=F32)


def grant(mib):
    return pltpu.CompilerParams(vmem_limit_bytes=mib << 20)


def cost(flops, nbytes):
    return pl.CostEstimate(flops=int(flops), bytes_accessed=int(nbytes), transcendentals=0)


def route_kernel(
    experts, cap, early, ids_ref, wts_ref, state_ref, cot_ref, sent_ref, pick_ref, late_ref, scale_ref
):
    tokens = ids_ref.shape[1]
    first, second = ids_ref[0:1, :], ids_ref[1:2, :]
    expert = lax.broadcasted_iota(jnp.int32, (experts, tokens), 0)
    is_first, is_second = first == expert, second == expert
    named = jnp.logical_or(is_first, is_second)
    before = lax.broadcasted_iota(jnp.int32, (tokens, tokens), 0) < lax.broadcasted_iota(
        jnp.int32, (tokens, tokens), 1
    )
    earlier = dot_nn(named.astype(F32).astype(BF16), before.astype(F32).astype(BF16))
    slot = jnp.where(named, earlier.astype(jnp.int32), -1)
    weight = jnp.where(is_first, wts_ref[0:1, :], jnp.where(is_second, wts_ref[1:2, :], 0.0))
    place = lax.broadcasted_iota(jnp.int32, (cap, tokens), 0)
    hits, scales = [], []
    for e in range(experts):
        hit = slot[e : e + 1, :] == place
        hits.append(hit.astype(F32))
        scales.append(jnp.sum(jnp.where(hit, weight[e : e + 1, :], 0.0), axis=1, keepdims=True))
    pick = jnp.concatenate(hits, axis=0).astype(BF16)
    pick_ref[...] = pick
    late_ref[...] = jnp.concatenate([hit[early:] for hit in hits], axis=0).astype(BF16)
    late_scale = jnp.concatenate([taken[early:] for taken in scales], axis=0)
    scale_ref[...] = jnp.broadcast_to(late_scale, scale_ref.shape)
    state_rows = dot_nn(pick, state_ref[...])
    soon = jnp.concatenate([hit[:early] for hit in hits], axis=0).astype(BF16)
    soon_rows = dot_nn(soon, cot_ref[...]) * jnp.concatenate(
        [taken[:early] for taken in scales], axis=0
    )
    both = []
    for e in range(experts):
        both += [state_rows[e * cap : (e + 1) * cap], soon_rows[e * early : (e + 1) * early]]
    sent_ref[...] = jnp.concatenate(both, axis=0).astype(BF16)


def spread_kernel(pick_ref, scale_ref, *refs):
    pieces, out_ref = refs[:-1], refs[-1]
    width = pieces[0].shape[1]
    scale = scale_ref[:, 0:1]
    for j, piece in enumerate(pieces):
        rows = (dot_nn(pick_ref[...], piece[...]) * scale).astype(BF16)
        out_ref[:, j * width : (j + 1) * width] = rows


def down_columns(slab_ref, base, wd_ref, count, width):
    pieces = [
        wd_ref[:, pl.ds(pl.multiple_of(slab_ref[base + j] * width, width), width)]
        for j in range(count)
    ]
    return jnp.concatenate(pieces, axis=1)


def expert_kernel(
    cap,
    early,
    slab_ref,
    state_ref,
    early_ref,
    ml_ref,
    mh_ref,
    tl_ref,
    th_ref,
    wg_ref,
    wu_ref,
    wd_ref,
    part_ref,
    act_ref,
    soon_ref,
    late_ref,
    wgu_ref,
    soon_back_ref,
):
    slabs, width = state_ref.shape[0], state_ref.shape[2]
    hidden_n = wd_ref.shape[0]

    @pl.when(pl.program_id(0) == 0)
    def _():
        wgu_ref[:hidden_n] = wg_ref[...]
        wgu_ref[hidden_n:] = wu_ref[...]
        soon = jnp.concatenate([early_ref[s] for s in range(slabs)], axis=1)
        soon_back_ref[...] = dot_nt(soon, wd_ref[...])

    rows = jnp.concatenate([state_ref[s] for s in range(slabs)], axis=1)
    pre = dot_nt(rows, wgu_ref[...])
    gate_pre, up_pre = pre[:, :hidden_n], pre[:, hidden_n:]
    per = ml_ref.shape[1] // width
    late = jnp.zeros((ml_ref.shape[0], hidden_n), F32)
    for q, ref in enumerate((ml_ref, mh_ref, tl_ref, th_ref)):
        late = late + dot_nt(ref[...], down_columns(slab_ref, q * per, wd_ref, per, width))
    late_n = cap - early
    groups = range(rows.shape[0] // cap)
    few = len(groups) * early
    soon_back = soon_back_ref[pl.ds(pl.multiple_of(pl.program_id(0) * few, few), few), :]
    back_hidden = jnp.concatenate(
        [
            x
            for i in groups
            for x in (
                soon_back[i * early : (i + 1) * early],
                late[i * late_n : (i + 1) * late_n],
            )
        ],
        axis=0,
    )
    sig_gate = jax.nn.sigmoid(gate_pre)
    silu_gate = gate_pre * sig_gate
    hidden = silu_gate * up_pre
    back_gate = (back_hidden * up_pre * sig_gate * (1.0 + gate_pre * (1.0 - sig_gate))).astype(BF16)
    back_up = (back_hidden * silu_gate).astype(BF16)
    back = jnp.concatenate([back_gate, back_up], axis=1)
    act_ref[...] = back
    soon_ref[...] = jnp.concatenate(
        [hidden[i * cap : i * cap + early] for i in groups], axis=0
    ).astype(BF16)
    late_ref[...] = jnp.concatenate(
        [hidden[i * cap + early : (i + 1) * cap] for i in groups], axis=0
    ).astype(BF16)
    for s in range(slabs):
        part_ref[s] = dot_nn(back, wgu_ref[:, s * width : (s + 1) * width]).astype(BF16)


def weight_grad_kernel(
    slab_ref,
    act_ref,
    soon_ref,
    late_ref,
    state_ref,
    early_ref,
    ml_ref,
    mh_ref,
    tl_ref,
    th_ref,
    gg_ref,
    gu_ref,
    gd_ref,
):
    hidden_n = gg_ref.shape[0]
    step, per = pl.program_id(0), pl.num_programs(0) // 4
    both = dot_tn(act_ref[...], state_ref[0])
    gg_ref[...] = both[:hidden_n]
    gu_ref[...] = both[hidden_n:]
    soon = dot_tn(soon_ref[...], early_ref[0])
    for q, ref in enumerate((ml_ref, mh_ref, tl_ref, th_ref)):

        @pl.when(step // per == q)
        def _(ref=ref):
            gd_ref[...] = soon + dot_tn(late_ref[...], ref[...])


def combine_kernel(pick_ref, rows_ref, cot_ref, out_ref):
    total = dot_tn(pick_ref[...], rows_ref[...])
    out_ref[...] = (cot_ref[...].astype(F32) + total).astype(BF16)


def proj_kernel(slab_ref, act_ref, *refs):
    pieces, out_ref = refs[:-1], refs[-1]
    for j, piece in enumerate(pieces):
        out_ref[slab_ref[j]] = dot_nn(act_ref[...], piece[...]).astype(BF16)


def mixer_kernel(slab_ref, proj_ref, conv_ref, outer_ref, *refs):
    pieces, (grad_ref, back_ref) = refs[:-2], refs[-2:]
    width = pieces[0].shape[1]
    back = jnp.zeros(back_ref.shape, F32)
    for j, piece in enumerate(pieces):
        start = pl.multiple_of(slab_ref[j] * width, width)
        back = back + dot_nt(proj_ref[:, pl.ds(start, width)], piece[...])
    grad_ref[...] = (back * conv_ref[...]).astype(BF16)
    back_ref[...] = back * outer_ref[...].astype(F32)


def ring_steps(size):
    steps = [0]
    for k in range(1, size // 2):
        steps += [k, -k]
    return steps + [size // 2]


def gathered(value, axis):
    size = lax.axis_size(axis)
    pieces = [value]
    for k in ring_steps(size)[1:]:
        pieces.append(lax.ppermute(value, axis, [(i, (i + k) % size) for i in range(size)]))
    return pieces


def from_behind(value, axis, steps):
    count = lax.axis_size(axis)
    first, last = (max(0, -steps), min(count, count - steps))
    return lax.ppermute(value, axis, [(source, source + steps) for source in range(first, last)])


def shards(
    conv_outer,
    conv_inner,
    conv_input,
    conv_taps,
    out_proj,
    mixed_state,
    route_ids,
    route_weights,
    w_gate,
    w_up,
    w_down,
    cotangent,
):
    tok_count, width = mixed_state.shape
    sp_size = lax.axis_size("sp")
    z_size = lax.axis_size("z")
    slabs = 2 * z_size
    local_experts, hidden_n, features = w_gate.shape
    experts = local_experts * sp_size
    cap = 4 * tok_count // experts
    slots = experts * cap
    core, place = lax.axis_index("c"), lax.axis_index("z")
    origin = (place - jnp.array(ring_steps(z_size), jnp.int32)) % z_size
    slab_of = jnp.concatenate([2 * origin + core, 2 * origin + 1 - core]).astype(jnp.int32)
    shape = jax.ShapeDtypeStruct

    cot_pieces = gathered(cotangent, "z")

    early = cap // 8
    late_n = cap - early
    own, late_rows, soon_rows = experts * (cap + early), experts * late_n, experts * early
    sent_rows, pick, late_pick, late_scale = pl.pallas_call(
        functools.partial(route_kernel, experts, cap, early),
        out_shape=(
            shape((own, width), BF16),
            shape((slots, tok_count), BF16),
            shape((late_rows, tok_count), BF16),
            shape((late_rows, 128), F32),
        ),
        cost_estimate=cost(2 * slots * tok_count * width, 4 * slots * width),
        name="route",
    )(route_ids.T, route_weights.T, mixed_state, cotangent)
    recv_rows = lax.all_to_all(
        sent_rows.reshape(experts, cap + early, width), "sp", split_axis=0, concat_axis=0, tiled=True
    )
    ordered = jnp.concatenate(
        [
            recv_rows[:, :cap].reshape(slots, width),
            recv_rows[:, cap:].reshape(soon_rows, width),
        ],
        axis=0,
    )
    state_all = lax.all_gather(ordered, TP, axis=0, tiled=False)

    half = z_size // 2 * width
    swap = [(0, 1), (1, 0)]

    def spread(pieces):
        return pl.pallas_call(
            spread_kernel,
            out_shape=shape((late_rows, half), BF16),
            cost_estimate=cost(2 * late_rows * tok_count * half, 4 * late_rows * half),
        )(late_pick, late_scale, *pieces)

    def exchanged(part):
        got = lax.all_to_all(
            part.reshape(experts, late_n, half), "sp", split_axis=0, concat_axis=0, tiled=True
        ).reshape(late_rows, half)
        return got, lax.ppermute(got, "c", swap)

    my_low, their_low = exchanged(spread(cot_pieces[: z_size // 2]))
    my_high, their_high = exchanged(spread(cot_pieces[z_size // 2 :]))
    cots = (my_low, my_high, their_low, their_high)

    steps = 4
    block = slots // steps
    whole = lambda *dims: pl.BlockSpec(dims, lambda *_: (0,) * len(dims))
    by_rows = lambda *dims: pl.BlockSpec(dims, lambda r, slab: (r, 0))
    partial_value, acts, soon_acts, late_acts = pl.pallas_call(
        functools.partial(expert_kernel, cap, early),
        grid_spec=pltpu.PrefetchScalarGridSpec(
            num_scalar_prefetch=1,
            grid=(steps,),
            in_specs=[
                pl.BlockSpec((slabs, block, width), lambda r, slab: (0, r, 0)),
                pl.BlockSpec((slabs, soon_rows, width), lambda r, slab: (0, slots // soon_rows, 0)),
                *[by_rows(late_rows // steps, half)] * 4,
                *[whole(hidden_n, features)] * 3,
            ],
            out_specs=[
                pl.BlockSpec((slabs, block, width), lambda r, slab: (0, r, 0)),
                by_rows(block, 2 * hidden_n),
                by_rows(soon_rows // steps, hidden_n),
                by_rows(late_rows // steps, hidden_n),
            ],
            scratch_shapes=[
                pltpu.VMEM((2 * hidden_n, features), BF16),
                pltpu.VMEM((soon_rows, hidden_n), F32),
            ],
        ),
        out_shape=(
            shape((slabs, slots, width), BF16),
            shape((slots, 2 * hidden_n), BF16),
            shape((soon_rows, hidden_n), BF16),
            shape((late_rows, hidden_n), BF16),
        ),
        cost_estimate=cost(10 * slots * hidden_n * features, 6 * slots * features),
        name="expert",
        compiler_params=grant(50),
    )(slab_of, state_all, state_all, *cots, w_gate[0], w_up[0], w_down[0])

    row_back = lax.psum_scatter(partial_value, TP, scatter_dimension=0, tiled=False)

    quarter = slabs // 4

    def cot_piece(q):
        return pl.BlockSpec(
            (late_rows, width), lambda s, slab: (0, jnp.clip(s - q * quarter, 0, quarter - 1))
        )

    grad_out = pl.BlockSpec((hidden_n, width), lambda s, slab: (0, slab[s]))
    grad_gate, grad_up, grad_down = pl.pallas_call(
        weight_grad_kernel,
        grid_spec=pltpu.PrefetchScalarGridSpec(
            num_scalar_prefetch=1,
            grid=(slabs,),
            in_specs=[
                whole(slots, 2 * hidden_n),
                whole(soon_rows, hidden_n),
                whole(late_rows, hidden_n),
                pl.BlockSpec((1, slots, width), lambda s, slab: (slab[s], 0, 0)),
                pl.BlockSpec((1, soon_rows, width), lambda s, slab: (slab[s], slots // soon_rows, 0)),
                *[cot_piece(q) for q in range(4)],
            ],
            out_specs=[grad_out] * 3,
        ),
        out_shape=(shape((hidden_n, features), F32),) * 3,
        cost_estimate=cost(6 * slots * hidden_n * features, 6 * slots * features),
        name="weight_grads",
    )(slab_of, acts, soon_acts, late_acts, state_all, state_all, *cots)
    row_back, grad_gate, grad_up, grad_down = lax.optimization_barrier(
        (row_back, grad_gate, grad_up, grad_down)
    )

    arrived = lax.all_to_all(
        row_back.reshape(experts, cap, width), "sp", split_axis=0, concat_axis=0, tiled=True
    ).reshape(slots, width)
    grad_mixed = pl.pallas_call(
        combine_kernel,
        out_shape=shape((tok_count, width), BF16),
        cost_estimate=cost(2 * slots * tok_count * width, 4 * slots * width),
        name="combine",
        compiler_params=grant(16),
    )(pick, arrived, cotangent)
    near = gathered(grad_mixed, "z")
    full_back = near + [lax.ppermute(piece, "c", swap) for piece in near]

    taps_count = conv_taps.shape[0]
    rim_width = taps_count - 1
    channels = conv_inner.shape[0]
    head_block = from_behind(
        jnp.stack([conv_inner[:, tok_count - rim_width :], conv_input[:, tok_count - rim_width :]]),
        "sp",
        1,
    )
    inner_ext = jnp.concatenate([head_block[0], conv_inner], axis=1).astype(F32)
    input_ext = jnp.concatenate([head_block[1], conv_input], axis=1).astype(F32)
    inner_prod = inner_ext * input_ext
    conv_out = jnp.zeros((channels, tok_count), F32)
    for offset in range(taps_count):
        conv_out = (
            conv_out + conv_taps[offset][:, None] * inner_prod[:, offset : offset + tok_count]
        )
    mixer_act = (conv_outer.astype(F32) * conv_out).astype(BF16)

    vmem, smem = pl.BlockSpec(memory_space=pltpu.VMEM), pl.BlockSpec(memory_space=pltpu.SMEM)
    proj_term = pl.pallas_call(
        proj_kernel,
        in_specs=[smem] + [vmem] * (1 + slabs),
        out_shape=shape((slabs, channels, width), BF16),
        cost_estimate=cost(2 * channels * tok_count * features, 4 * tok_count * features),
        name="proj",
    )(slab_of, mixer_act, *full_back)
    landed = lax.all_to_all(proj_term, "sp", split_axis=0, concat_axis=0, tiled=True)
    grad_proj = jnp.sum(landed.astype(F32), axis=0)
    grad_outer, back_conv = pl.pallas_call(
        mixer_kernel,
        in_specs=[smem] + [vmem] * (3 + slabs),
        out_shape=(shape((channels, tok_count), BF16), shape((channels, tok_count), F32)),
        cost_estimate=cost(2 * channels * tok_count * features, 4 * tok_count * features),
        name="mixer",
    )(slab_of, out_proj, conv_out, conv_outer, *full_back)
    tail_back = from_behind(back_conv[:, :rim_width], "sp", -1)
    back_ext = jnp.concatenate([back_conv, tail_back], axis=1)
    back_prod = jnp.zeros_like(back_conv)
    for offset in range(taps_count):
        shift_by = rim_width - offset
        back_prod = (
            back_prod + conv_taps[offset][:, None] * back_ext[:, shift_by : shift_by + tok_count]
        )
    grad_inner = (back_prod * conv_input.astype(F32)).astype(BF16)
    grad_input = (back_prod * conv_inner.astype(F32)).astype(BF16)
    return (
        grad_gate[None],
        grad_up[None],
        grad_down[None],
        grad_mixed,
        grad_proj,
        grad_outer,
        grad_inner,
        grad_input,
    )


def solution(mesh):
    torus = Mesh(mesh.devices.reshape(mesh.shape["sp"], mesh.shape["tp"] // 2, 2), ("sp", "z", "c"))

    return jax.shard_map(
        shards,
        mesh=torus,
        in_specs=(
            P(TP, "sp"),
            P(TP, "sp"),
            P(TP, "sp"),
            P(None, TP),
            P(TP, None),
            P("sp", TP),
            P("sp", None),
            P("sp", None),
            P("sp", TP, None),
            P("sp", TP, None),
            P("sp", TP, None),
            P("sp", TP),
        ),
        out_specs=(
            P("sp", TP, None),
            P("sp", TP, None),
            P("sp", TP, None),
            P("sp", TP),
            P(TP, "sp"),
            P(TP, "sp"),
            P(TP, "sp"),
            P(TP, "sp"),
        ),
        check_vma=False,
    )
```

```python
import functools

import jax
import jax.numpy as jnp
from jax import lax
from jax.experimental import pallas as pl
from jax.experimental.pallas import tpu as pltpu
from jax.sharding import Mesh
from jax.sharding import PartitionSpec as P


TP = ("z", "c")
BF16 = jnp.bfloat16
F32 = jnp.float32


def dot_nn(a, b):
    return lax.dot_general(a, b, (((1,), (0,)), ((), ())), preferred_element_type=F32)


def dot_nt(a, b):
    return lax.dot_general(a, b, (((1,), (1,)), ((), ())), preferred_element_type=F32)


def dot_tn(a, b):
    return lax.dot_general(a, b, (((0,), (0,)), ((), ())), preferred_element_type=F32)


def grant(mib):
    return pltpu.CompilerParams(vmem_limit_bytes=mib << 20)


def cost(flops, nbytes):
    return pl.CostEstimate(flops=int(flops), bytes_accessed=int(nbytes), transcendentals=0)


def route_kernel(
    experts, cap, early, ids_ref, wts_ref, state_ref, cot_ref, sent_ref, pick_ref, late_ref, scale_ref
):
    tokens = ids_ref.shape[1]
    first, second = ids_ref[0:1, :], ids_ref[1:2, :]
    expert = lax.broadcasted_iota(jnp.int32, (experts, tokens), 0)
    is_first, is_second = first == expert, second == expert
    named = jnp.logical_or(is_first, is_second)
    before = lax.broadcasted_iota(jnp.int32, (tokens, tokens), 0) < lax.broadcasted_iota(
        jnp.int32, (tokens, tokens), 1
    )
    earlier = dot_nn(named.astype(F32).astype(BF16), before.astype(F32).astype(BF16))
    slot = jnp.where(named, earlier.astype(jnp.int32), -1)
    weight = jnp.where(is_first, wts_ref[0:1, :], jnp.where(is_second, wts_ref[1:2, :], 0.0))
    place = lax.broadcasted_iota(jnp.int32, (cap, tokens), 0)
    hits, scales = [], []
    for e in range(experts):
        hit = slot[e : e + 1, :] == place
        hits.append(hit.astype(F32))
        scales.append(jnp.sum(jnp.where(hit, weight[e : e + 1, :], 0.0), axis=1, keepdims=True))
    pick = jnp.concatenate(hits, axis=0).astype(BF16)
    pick_ref[...] = pick
    late_ref[...] = jnp.concatenate([hit[early:] for hit in hits], axis=0).astype(BF16)
    late_scale = jnp.concatenate([taken[early:] for taken in scales], axis=0)
    scale_ref[...] = jnp.broadcast_to(late_scale, scale_ref.shape)
    state_rows = dot_nn(pick, state_ref[...])
    soon = jnp.concatenate([hit[:early] for hit in hits], axis=0).astype(BF16)
    soon_rows = dot_nn(soon, cot_ref[...]) * jnp.concatenate(
        [taken[:early] for taken in scales], axis=0
    )
    both = []
    for e in range(experts):
        both += [state_rows[e * cap : (e + 1) * cap], soon_rows[e * early : (e + 1) * early]]
    sent_ref[...] = jnp.concatenate(both, axis=0).astype(BF16)


def spread_kernel(pick_ref, scale_ref, *refs):
    pieces, out_ref = refs[:-1], refs[-1]
    width = pieces[0].shape[1]
    scale = scale_ref[:, 0:1]
    for j, piece in enumerate(pieces):
        rows = (dot_nn(pick_ref[...], piece[...]) * scale).astype(BF16)
        out_ref[:, j * width : (j + 1) * width] = rows


def down_columns(slab_ref, base, wd_ref, count, width):
    pieces = [
        wd_ref[:, pl.ds(pl.multiple_of(slab_ref[base + j] * width, width), width)]
        for j in range(count)
    ]
    return jnp.concatenate(pieces, axis=1)


def expert_kernel(
    cap,
    early,
    slab_ref,
    state_ref,
    early_ref,
    ml_ref,
    mh_ref,
    tl_ref,
    th_ref,
    wg_ref,
    wu_ref,
    wd_ref,
    part_ref,
    act_ref,
    soon_ref,
    late_ref,
    wgu_ref,
    soon_back_ref,
):
    slabs, width = state_ref.shape[0], state_ref.shape[2]
    hidden_n = wd_ref.shape[0]

    @pl.when(pl.program_id(0) == 0)
    def _():
        wgu_ref[:hidden_n] = wg_ref[...]
        wgu_ref[hidden_n:] = wu_ref[...]
        soon = jnp.concatenate([early_ref[s] for s in range(slabs)], axis=1)
        soon_back_ref[...] = dot_nt(soon, wd_ref[...])

    rows = jnp.concatenate([state_ref[s] for s in range(slabs)], axis=1)
    pre = dot_nt(rows, wgu_ref[...])
    gate_pre, up_pre = pre[:, :hidden_n], pre[:, hidden_n:]
    per = ml_ref.shape[1] // width
    late = jnp.zeros((ml_ref.shape[0], hidden_n), F32)
    for q, ref in enumerate((ml_ref, mh_ref, tl_ref, th_ref)):
        late = late + dot_nt(ref[...], down_columns(slab_ref, q * per, wd_ref, per, width))
    late_n = cap - early
    groups = range(rows.shape[0] // cap)
    few = len(groups) * early
    soon_back = soon_back_ref[pl.ds(pl.multiple_of(pl.program_id(0) * few, few), few), :]
    back_hidden = jnp.concatenate(
        [
            x
            for i in groups
            for x in (
                soon_back[i * early : (i + 1) * early],
                late[i * late_n : (i + 1) * late_n],
            )
        ],
        axis=0,
    )
    sig_gate = jax.nn.sigmoid(gate_pre)
    silu_gate = gate_pre * sig_gate
    hidden = silu_gate * up_pre
    back_gate = (back_hidden * up_pre * sig_gate * (1.0 + gate_pre * (1.0 - sig_gate))).astype(BF16)
    back_up = (back_hidden * silu_gate).astype(BF16)
    back = jnp.concatenate([back_gate, back_up], axis=1)
    act_ref[...] = back
    soon_ref[...] = jnp.concatenate(
        [hidden[i * cap : i * cap + early] for i in groups], axis=0
    ).astype(BF16)
    late_ref[...] = jnp.concatenate(
        [hidden[i * cap + early : (i + 1) * cap] for i in groups], axis=0
    ).astype(BF16)
    for s in range(slabs):
        part_ref[s] = dot_nn(back, wgu_ref[:, s * width : (s + 1) * width]).astype(BF16)


def weight_grad_kernel(
    slab_ref,
    act_ref,
    soon_ref,
    late_ref,
    state_ref,
    early_ref,
    ml_ref,
    mh_ref,
    tl_ref,
    th_ref,
    gg_ref,
    gu_ref,
    gd_ref,
):
    hidden_n = gg_ref.shape[0]
    step, per = pl.program_id(0), pl.num_programs(0) // 4
    both = dot_tn(act_ref[...], state_ref[0])
    gg_ref[...] = both[:hidden_n]
    gu_ref[...] = both[hidden_n:]
    soon = dot_tn(soon_ref[...], early_ref[0])
    for q, ref in enumerate((ml_ref, mh_ref, tl_ref, th_ref)):

        @pl.when(step // per == q)
        def _(ref=ref):
            gd_ref[...] = soon + dot_tn(late_ref[...], ref[...])


def combine_kernel(pick_ref, rows_ref, cot_ref, out_ref):
    total = dot_tn(pick_ref[...], rows_ref[...])
    out_ref[...] = (cot_ref[...].astype(F32) + total).astype(BF16)


def proj_kernel(slab_ref, act_ref, *refs):
    pieces, out_ref = refs[:-1], refs[-1]
    for j, piece in enumerate(pieces):
        out_ref[slab_ref[j]] = dot_nn(act_ref[...], piece[...]).astype(BF16)


def mixer_kernel(slab_ref, proj_ref, conv_ref, outer_ref, *refs):
    pieces, (grad_ref, back_ref) = refs[:-2], refs[-2:]
    width = pieces[0].shape[1]
    back = jnp.zeros(back_ref.shape, F32)
    for j, piece in enumerate(pieces):
        start = pl.multiple_of(slab_ref[j] * width, width)
        back = back + dot_nt(proj_ref[:, pl.ds(start, width)], piece[...])
    grad_ref[...] = (back * conv_ref[...]).astype(BF16)
    back_ref[...] = back * outer_ref[...].astype(F32)


def ring_steps(size):
    steps = [0]
    for k in range(1, size // 2):
        steps += [k, -k]
    return steps + [size // 2]


def gathered(value, axis):
    size = lax.axis_size(axis)
    pieces = [value]
    for k in ring_steps(size)[1:]:
        pieces.append(lax.ppermute(value, axis, [(i, (i + k) % size) for i in range(size)]))
    return pieces


def from_behind(value, axis, steps):
    count = lax.axis_size(axis)
    first, last = (max(0, -steps), min(count, count - steps))
    return lax.ppermute(value, axis, [(source, source + steps) for source in range(first, last)])


def shards(
    conv_outer,
    conv_inner,
    conv_input,
    conv_taps,
    out_proj,
    mixed_state,
    route_ids,
    route_weights,
    w_gate,
    w_up,
    w_down,
    cotangent,
):
    tok_count, width = mixed_state.shape
    sp_size = lax.axis_size("sp")
    z_size = lax.axis_size("z")
    slabs = 2 * z_size
    local_experts, hidden_n, features = w_gate.shape
    experts = local_experts * sp_size
    cap = 4 * tok_count // experts
    slots = experts * cap
    core, place = lax.axis_index("c"), lax.axis_index("z")
    origin = (place - jnp.array(ring_steps(z_size), jnp.int32)) % z_size
    slab_of = jnp.concatenate([2 * origin + core, 2 * origin + 1 - core]).astype(jnp.int32)
    shape = jax.ShapeDtypeStruct

    cot_pieces = gathered(cotangent, "z")

    early = cap // 8
    late_n = cap - early
    own, late_rows, soon_rows = experts * (cap + early), experts * late_n, experts * early
    sent_rows, pick, late_pick, late_scale = pl.pallas_call(
        functools.partial(route_kernel, experts, cap, early),
        out_shape=(
            shape((own, width), BF16),
            shape((slots, tok_count), BF16),
            shape((late_rows, tok_count), BF16),
            shape((late_rows, 128), F32),
        ),
        cost_estimate=cost(2 * slots * tok_count * width, 4 * slots * width),
        name="route",
    )(route_ids.T, route_weights.T, mixed_state, cotangent)
    recv_rows = lax.all_to_all(
        sent_rows.reshape(experts, cap + early, width), "sp", split_axis=0, concat_axis=0, tiled=True
    )
    ordered = jnp.concatenate(
        [
            recv_rows[:, :cap].reshape(slots, width),
            recv_rows[:, cap:].reshape(soon_rows, width),
        ],
        axis=0,
    )
    state_all = lax.all_gather(ordered, TP, axis=0, tiled=False)

    half = z_size // 2 * width
    swap = [(0, 1), (1, 0)]

    def spread(pieces):
        return pl.pallas_call(
            spread_kernel,
            out_shape=shape((late_rows, half), BF16),
            cost_estimate=cost(2 * late_rows * tok_count * half, 4 * late_rows * half),
        )(late_pick, late_scale, *pieces)

    def exchanged(part):
        got = lax.all_to_all(
            part.reshape(experts, late_n, half), "sp", split_axis=0, concat_axis=0, tiled=True
        ).reshape(late_rows, half)
        return got, lax.ppermute(got, "c", swap)

    my_low, their_low = exchanged(spread(cot_pieces[: z_size // 2]))
    my_high, their_high = exchanged(spread(cot_pieces[z_size // 2 :]))
    cots = (my_low, my_high, their_low, their_high)

    steps = 4
    block = slots // steps
    whole = lambda *dims: pl.BlockSpec(dims, lambda *_: (0,) * len(dims))
    by_rows = lambda *dims: pl.BlockSpec(dims, lambda r, slab: (r, 0))
    partial_value, acts, soon_acts, late_acts = pl.pallas_call(
        functools.partial(expert_kernel, cap, early),
        grid_spec=pltpu.PrefetchScalarGridSpec(
            num_scalar_prefetch=1,
            grid=(steps,),
            in_specs=[
                pl.BlockSpec((slabs, block, width), lambda r, slab: (0, r, 0)),
                pl.BlockSpec((slabs, soon_rows, width), lambda r, slab: (0, slots // soon_rows, 0)),
                *[by_rows(late_rows // steps, half)] * 4,
                *[whole(hidden_n, features)] * 3,
            ],
            out_specs=[
                pl.BlockSpec((slabs, block, width), lambda r, slab: (0, r, 0)),
                by_rows(block, 2 * hidden_n),
                by_rows(soon_rows // steps, hidden_n),
                by_rows(late_rows // steps, hidden_n),
            ],
            scratch_shapes=[
                pltpu.VMEM((2 * hidden_n, features), BF16),
                pltpu.VMEM((soon_rows, hidden_n), F32),
            ],
        ),
        out_shape=(
            shape((slabs, slots, width), BF16),
            shape((slots, 2 * hidden_n), BF16),
            shape((soon_rows, hidden_n), BF16),
            shape((late_rows, hidden_n), BF16),
        ),
        cost_estimate=cost(10 * slots * hidden_n * features, 6 * slots * features),
        name="expert",
    )(slab_of, state_all, state_all, *cots, w_gate[0], w_up[0], w_down[0])

    row_back = lax.psum_scatter(partial_value, TP, scatter_dimension=0, tiled=False)

    quarter = slabs // 4

    def cot_piece(q):
        return pl.BlockSpec(
            (late_rows, width), lambda s, slab: (0, jnp.clip(s - q * quarter, 0, quarter - 1))
        )

    grad_out = pl.BlockSpec((hidden_n, width), lambda s, slab: (0, slab[s]))
    grad_gate, grad_up, grad_down = pl.pallas_call(
        weight_grad_kernel,
        grid_spec=pltpu.PrefetchScalarGridSpec(
            num_scalar_prefetch=1,
            grid=(slabs,),
            in_specs=[
                whole(slots, 2 * hidden_n),
                whole(soon_rows, hidden_n),
                whole(late_rows, hidden_n),
                pl.BlockSpec((1, slots, width), lambda s, slab: (slab[s], 0, 0)),
                pl.BlockSpec((1, soon_rows, width), lambda s, slab: (slab[s], slots // soon_rows, 0)),
                *[cot_piece(q) for q in range(4)],
            ],
            out_specs=[grad_out] * 3,
        ),
        out_shape=(shape((hidden_n, features), F32),) * 3,
        cost_estimate=cost(6 * slots * hidden_n * features, 6 * slots * features),
        name="weight_grads",
    )(slab_of, acts, soon_acts, late_acts, state_all, state_all, *cots)
    taps_count = conv_taps.shape[0]
    rim_width = taps_count - 1
    channels = conv_inner.shape[0]
    head_block = from_behind(
        jnp.stack([conv_inner[:, tok_count - rim_width :], conv_input[:, tok_count - rim_width :]]),
        "sp",
        1,
    )
    inner_ext = jnp.concatenate([head_block[0], conv_inner], axis=1).astype(F32)
    input_ext = jnp.concatenate([head_block[1], conv_input], axis=1).astype(F32)
    inner_prod = inner_ext * input_ext
    conv_out = jnp.zeros((channels, tok_count), F32)
    for offset in range(taps_count):
        conv_out = (
            conv_out + conv_taps[offset][:, None] * inner_prod[:, offset : offset + tok_count]
        )
    mixer_act = (conv_outer.astype(F32) * conv_out).astype(BF16)

    row_back, grad_gate, grad_up, grad_down, conv_out, mixer_act = lax.optimization_barrier(
        (row_back, grad_gate, grad_up, grad_down, conv_out, mixer_act)
    )

    arrived = lax.all_to_all(
        row_back.reshape(experts, cap, width), "sp", split_axis=0, concat_axis=0, tiled=True
    ).reshape(slots, width)
    grad_mixed = pl.pallas_call(
        combine_kernel,
        out_shape=shape((tok_count, width), BF16),
        cost_estimate=cost(2 * slots * tok_count * width, 4 * slots * width),
        name="combine",
        compiler_params=grant(16),
    )(pick, arrived, cotangent)
    near = gathered(grad_mixed, "z")
    full_back = near + [lax.ppermute(piece, "c", swap) for piece in near]

    vmem, smem = pl.BlockSpec(memory_space=pltpu.VMEM), pl.BlockSpec(memory_space=pltpu.SMEM)
    proj_term = pl.pallas_call(
        proj_kernel,
        in_specs=[smem] + [vmem] * (1 + slabs),
        out_shape=shape((slabs, channels, width), BF16),
        cost_estimate=cost(2 * channels * tok_count * features, 4 * tok_count * features),
        name="proj",
    )(slab_of, mixer_act, *full_back)
    landed = lax.all_to_all(proj_term, "sp", split_axis=0, concat_axis=0, tiled=True)
    grad_proj = jnp.sum(landed.astype(F32), axis=0)
    grad_outer, back_conv = pl.pallas_call(
        mixer_kernel,
        in_specs=[smem] + [vmem] * (3 + slabs),
        out_shape=(shape((channels, tok_count), BF16), shape((channels, tok_count), F32)),
        cost_estimate=cost(2 * channels * tok_count * features, 4 * tok_count * features),
        name="mixer",
    )(slab_of, out_proj, conv_out, conv_outer, *full_back)
    tail_back = from_behind(back_conv[:, :rim_width], "sp", -1)
    back_ext = jnp.concatenate([back_conv, tail_back], axis=1)
    back_prod = jnp.zeros_like(back_conv)
    for offset in range(taps_count):
        shift_by = rim_width - offset
        back_prod = (
            back_prod + conv_taps[offset][:, None] * back_ext[:, shift_by : shift_by + tok_count]
        )
    grad_inner = (back_prod * conv_input.astype(F32)).astype(BF16)
    grad_input = (back_prod * conv_inner.astype(F32)).astype(BF16)
    return (
        grad_gate[None],
        grad_up[None],
        grad_down[None],
        grad_mixed,
        grad_proj,
        grad_outer,
        grad_inner,
        grad_input,
    )


def solution(mesh):
    torus = Mesh(mesh.devices.reshape(mesh.shape["sp"], mesh.shape["tp"] // 2, 2), ("sp", "z", "c"))

    return jax.shard_map(
        shards,
        mesh=torus,
        in_specs=(
            P(TP, "sp"),
            P(TP, "sp"),
            P(TP, "sp"),
            P(None, TP),
            P(TP, None),
            P("sp", TP),
            P("sp", None),
            P("sp", None),
            P("sp", TP, None),
            P("sp", TP, None),
            P("sp", TP, None),
            P("sp", TP),
        ),
        out_specs=(
            P("sp", TP, None),
            P("sp", TP, None),
            P("sp", TP, None),
            P("sp", TP),
            P(TP, "sp"),
            P(TP, "sp"),
            P(TP, "sp"),
            P(TP, "sp"),
        ),
        check_vma=False,
    )
```
